256 devices in a mesh: sp: 32 (over z, x), tp: 8 (over y, core).
Axes of the slice: x: 4, y: 4, z: 8, core: 2. Of those that a mesh axis runs over, the one named last changes fastest.
Arguments:
- tokens: bfloat16 [16384, 2048], P(('sp', 'tp')), may hold values from -6 to 6
- input_gain: bfloat16 [2048], replicated, may hold values from 0.099609375 to 1.8984375
- weight_query: bfloat16 [2048, 1024], P(None, 'tp'), may hold values from -0.125 to 0.125
- weight_key: bfloat16 [2048, 1024], P(None, 'tp'), may hold values from -0.125 to 0.125
- weight_value: bfloat16 [2048, 2048], P(None, 'tp'), may hold values from -8 to 8
- weight_outgate: bfloat16 [2048, 2048], P(None, 'tp'), may hold values from -0.125 to 0.125
- weight_ingate: bfloat16 [2048, 8], replicated, may hold values from -0.125 to 0.125
- weight_forget: bfloat16 [2048, 8], replicated, may hold values from -0.125 to 0.125
- forget_shift: float32 [16384, 8], P('sp', 'tp'), may hold values from 0 to 20
- mem_gain: bfloat16 [2048], replicated, may hold values from 0.099609375 to 1.8984375
- query_down_weight: bfloat16 [2048, 768], P(None, 'tp'), may hold values from -0.125 to 0.125
- latent_down_weight: bfloat16 [2048, 512], P(None, 'tp'), may hold values from -0.125 to 0.125
- down_rotary: bfloat16 [2048, 64], replicated, may hold values from -0.125 to 0.125
- query_gain: float32 [768], replicated, may hold values from 0.15 to 12
- latent_gain: float32 [512], replicated, may hold values from 0.15 to 12
- query_up_weight: bfloat16 [768, 1536], P(None, 'tp'), may hold values from -0.4375 to 0.4375
- key_up_weight: bfloat16 [512, 1024], P(None, 'tp'), may hold values from -0.25 to 0.25
- value_up_weight: bfloat16 [512, 1024], P(None, 'tp'), may hold values from -0.25 to 0.25
- out_memory: bfloat16 [2048, 2048], P('tp'), may hold values from -0.5 to 0.5
- out_attend: bfloat16 [1024, 2048], P('tp'), may hold values from -0.75 to 0.75
Outputs:
- mixed: bfloat16 [16384, 2048], P(('sp', 'tp'))
The draws below stay inside these ranges and needn't reach their ends.
All inputs are finite; a program needn't handle non-finite values.
Results may differ from the reference program's by a relative error of at most 0.04.
The reference program's roundings to bfloat16 on the way count: a program that leaves them out, or rounds other values in their place, can miss the bound.
Values may be sent and summed in bfloat16 or wider, within the bound.
No kernel may reach another device: no remote copies, remote signals or barrier semaphores. Data moves between devices by JAX's collectives and lax.ppermute only.
A program may use at most 128 MiB of HBM per device.

```python
import jax
import jax.numpy as jnp
from jax import lax

MODEL_WIDTH = 2048
MEMORY_HEADS = 8
M_QK = 128
M_V = 256
ATTEND_HEADS = 8
PLAIN_CHANNELS = 128
ROTARY_CHANNELS = 64
VALUE_CHANNELS = 128
QUERY_LATENT = 768
LATENT_WIDTH = 512
BLOCK = 64
TOK_DEV = 512
SEQUENCE_LENGTH = 16384
N_TP = 8


def draw_forget_shift(key, part):
    random_keys = jax.random.split(key, 5)
    shuffled = jax.random.permutation(random_keys[0], MEMORY_HEADS)
    quick_heads = shuffled[:MEMORY_HEADS // 2]
    fast_head = jnp.any(jnp.arange(MEMORY_HEADS)[None, :] == quick_heads[:, None], axis=0)
    block_total = SEQUENCE_LENGTH // TOK_DEV
    factor = jnp.exp(jax.random.uniform(random_keys[1], (block_total, MEMORY_HEADS), jnp.float32, -0.7, 0.7))
    factor = jnp.repeat(factor, TOK_DEV, axis=0)
    jitter = jnp.exp(jax.random.uniform(random_keys[2], (SEQUENCE_LENGTH, MEMORY_HEADS), jnp.float32, -0.35, 0.35))
    decay_rate = jnp.where(fast_head[None, :], 1.0 / 40.0, 0.4 / SEQUENCE_LENGTH) * factor * jitter
    score_retained = -jnp.log(jnp.expm1(decay_rate))
    spike_position = jax.random.randint(random_keys[3], (4, MEMORY_HEADS), 0, SEQUENCE_LENGTH)
    spike_retained = jax.random.uniform(random_keys[4], (4, MEMORY_HEADS), jnp.float32, 0.5, 0.8)
    spike_score = jnp.log(spike_retained / (1.0 - spike_retained))
    spike_matches = jnp.arange(SEQUENCE_LENGTH)[:, None, None] == spike_position[None, :, :]
    spike_amount = jnp.min(jnp.where(spike_matches, spike_score[None], 1000000000.0), axis=1)
    score_retained = jnp.minimum(score_retained, spike_amount)
    ratio = jnp.clip(score_retained, 0.0, 13.5) / 15.0
    return 7.5 * jnp.log((1.0 + ratio) / (1.0 - ratio))


def gain_entries(key, length):
    return 1.0 + 0.18 * jnp.clip(jax.random.normal(key, (length,), jnp.float32), -4.5, 4.5)


def draw_query_gain(key, part):
    return gain_entries(jax.random.fold_in(key, 11), QUERY_LATENT)


def draw_latent_gain(key, part):
    return gain_entries(jax.random.fold_in(key, 23), LATENT_WIDTH)


def draw_weight_value(key, part):
    position = jnp.arange(MEMORY_HEADS, dtype=jnp.float32) / max(MEMORY_HEADS - 1, 1)
    top_scale = 3.0
    head_scale = jnp.repeat(jnp.power(top_scale, position), M_V)
    base = jnp.clip(jax.random.normal(jax.random.fold_in(key, 37), (MODEL_WIDTH, MEMORY_HEADS * M_V), jnp.float32), -6.0, 6.0)
    return (base * head_scale[None, :] * MODEL_WIDTH ** (-0.5)).astype(jnp.bfloat16)


def levels(key, shape, pieces, low, largest):
    level = 1.0
    for dim, parts in pieces:
        draws = jax.random.uniform(jax.random.fold_in(jax.random.fold_in(key, 6), dim), (parts,), jnp.float32, low / len(pieces), largest / len(pieces))
        level = level * jnp.repeat(jnp.exp(draws), shape[dim] // parts).reshape((-1,) + (1,) * (len(shape) - 1 - dim))
    return level


def bell_draw(key, dims, spread, most, shards=(), kind=jnp.bfloat16):
    level = levels(key, dims, shards, -0.22, 0.18) if shards else 1.0
    values = jax.random.normal(key, dims, jnp.float32) * spread * level
    return jnp.minimum(jnp.maximum(values, -most), most).astype(kind)


def setup_inputs(seed: int = 0) -> dict:
    key_list = jax.random.split(jax.random.key(seed), 21)
    tokens = bell_draw(key_list[0], (SEQUENCE_LENGTH, MODEL_WIDTH), 1.0, 6.0, ((0, 256),))
    input_gain = jnp.clip(1.0 + 0.18 * jax.random.normal(key_list[1], (MODEL_WIDTH,), jnp.float32), 0.099609375, 1.8984375).astype(jnp.bfloat16)
    weight_query = bell_draw(key_list[2], (MODEL_WIDTH, MEMORY_HEADS * M_QK), MODEL_WIDTH ** -0.5, 0.125, ((1, 8),))
    weight_key = bell_draw(key_list[3], (MODEL_WIDTH, MEMORY_HEADS * M_QK), MODEL_WIDTH ** -0.5, 0.125, ((1, 8),))
    weight_value = draw_weight_value(jax.random.fold_in(key_list[20], 71), 0)
    weight_outgate = bell_draw(key_list[5], (MODEL_WIDTH, MEMORY_HEADS * M_V), MODEL_WIDTH ** -0.5, 0.125, ((1, 8),))
    weight_ingate = bell_draw(key_list[6], (MODEL_WIDTH, MEMORY_HEADS), MODEL_WIDTH ** -0.5, 0.125)
    weight_forget = bell_draw(key_list[7], (MODEL_WIDTH, MEMORY_HEADS), MODEL_WIDTH ** -0.5, 0.125)
    forget_shift = draw_forget_shift(jax.random.fold_in(key_list[20], 71), 0)
    mem_gain = jnp.clip(1.0 + 0.18 * jax.random.normal(key_list[9], (MEMORY_HEADS * M_V,), jnp.float32), 0.099609375, 1.8984375).astype(jnp.bfloat16)
    query_down_weight = bell_draw(key_list[10], (MODEL_WIDTH, QUERY_LATENT), MODEL_WIDTH ** -0.5, 0.125, ((1, 8),))
    latent_down_weight = bell_draw(key_list[11], (MODEL_WIDTH, LATENT_WIDTH), MODEL_WIDTH ** -0.5, 0.125, ((1, 8),))
    down_rotary = bell_draw(key_list[12], (MODEL_WIDTH, ROTARY_CHANNELS), MODEL_WIDTH ** -0.5, 0.125)
    query_gain = draw_query_gain(jax.random.fold_in(key_list[20], 71), 0)
    latent_gain = draw_latent_gain(jax.random.fold_in(key_list[20], 71), 0)
    query_up_weight = bell_draw(key_list[15], (QUERY_LATENT, ATTEND_HEADS * (PLAIN_CHANNELS + ROTARY_CHANNELS)), (QUERY_LATENT // 4) ** -0.5, 0.4375, ((1, 8),))
    key_up_weight = bell_draw(key_list[16], (LATENT_WIDTH, ATTEND_HEADS * PLAIN_CHANNELS), LATENT_WIDTH ** -0.5, 0.25, ((1, 8),))
    value_up_weight = bell_draw(key_list[17], (LATENT_WIDTH, ATTEND_HEADS * VALUE_CHANNELS), LATENT_WIDTH ** -0.5, 0.25, ((1, 8),))
    out_memory = bell_draw(key_list[18], (MEMORY_HEADS * M_V, MODEL_WIDTH), (MEMORY_HEADS * M_V // 16) ** -0.5, 0.5, ((0, 8),))
    out_attend = bell_draw(key_list[19], (ATTEND_HEADS * VALUE_CHANNELS, MODEL_WIDTH), (ATTEND_HEADS * VALUE_CHANNELS // 16) ** -0.5, 0.75, ((0, 8),))
    return dict(tokens=tokens, input_gain=input_gain, weight_query=weight_query, weight_key=weight_key, weight_value=weight_value, weight_outgate=weight_outgate, weight_ingate=weight_ingate, weight_forget=weight_forget, forget_shift=forget_shift, mem_gain=mem_gain, query_down_weight=query_down_weight, latent_down_weight=latent_down_weight, down_rotary=down_rotary, query_gain=query_gain, latent_gain=latent_gain, query_up_weight=query_up_weight, key_up_weight=key_up_weight, value_up_weight=value_up_weight, out_memory=out_memory, out_attend=out_attend)


SMALL_CONSTANT = 1e-06
SOFTCAP = 15.0
ROTARY_BASE = 10000.0
PRECISE = lax.Precision.HIGHEST

def rms_scale(values, gain):
    widened = values.astype(jnp.float32)
    return widened * lax.rsqrt(lax.optimization_barrier(jnp.mean(widened * widened, axis=-1, keepdims=True)) + SMALL_CONSTANT) * gain.astype(jnp.float32)

def rotate(values, positions):
    halfway = values.shape[-1] // 2
    inverse = jnp.power(ROTARY_BASE, -jnp.arange(halfway, dtype=jnp.float32) / halfway)
    angles = positions.astype(jnp.float32)[:, None] * inverse
    cosine = jnp.cos(angles)
    sine_part = jnp.sin(angles)
    if values.ndim == 3:
        cosine = cosine[:, None, :]
        sine_part = sine_part[:, None, :]
    widened = values.astype(jnp.float32)
    first = widened[..., :halfway]
    second = widened[..., halfway:]
    turned = jnp.concatenate([first * cosine - second * sine_part, second * cosine + first * sine_part], axis=-1)
    return turned.astype(jnp.bfloat16)

def update_state(carried, key_rows, value_rows, input_gate, cumulative):
    matrix, normal, stabilizer = carried
    last_total = cumulative[:, -1]
    weight_log = last_total[:, None] - cumulative + input_gate
    new_max = jnp.maximum(last_total + stabilizer, lax.optimization_barrier(jnp.max(weight_log, axis=-1)))
    weights = jnp.exp(weight_log - new_max[:, None])
    decay = jnp.exp(last_total + stabilizer - new_max)
    matrix = decay[:, None, None] * matrix + jnp.einsum('hsv,hsd->hvd', weights[:, :, None] * value_rows, key_rows, precision=PRECISE)
    normal = decay[:, None] * normal + jnp.einsum('hs,hsd->hd', weights, key_rows, precision=PRECISE)
    return (matrix, normal, new_max)

def block_step(carried, inputs):
    query_rows, key_rows, value_rows, input_gate, log_forget = inputs
    matrix, normal, stabilizer = carried
    cumulative = jnp.cumsum(log_forget, axis=-1)
    block_len = log_forget.shape[-1]
    causal = jnp.tril(jnp.ones((block_len, block_len), dtype=bool))
    pair_log = cumulative[:, :, None] - cumulative[:, None, :] + input_gate[:, None, :]
    pair_log = jnp.where(causal, pair_log, -jnp.inf)
    carried_log = cumulative + stabilizer[:, None]
    row_max = jnp.maximum(carried_log, lax.optimization_barrier(jnp.max(pair_log, axis=-1)))
    within = jnp.exp(pair_log - row_max[:, :, None])
    across = jnp.exp(carried_log - row_max)
    affinity = jnp.einsum('hjd,hsd->hjs', query_rows, key_rows, precision=PRECISE) * within
    numerator = jnp.einsum('hjs,hsv->hjv', affinity, value_rows, precision=PRECISE)
    numerator = numerator + across[:, :, None] * jnp.einsum('hjd,hvd->hjv', query_rows, matrix, precision=PRECISE)
    denominator = lax.optimization_barrier(jnp.sum(affinity, axis=-1)) + across * jnp.einsum('hjd,hd->hj', query_rows, normal, precision=PRECISE)
    output = numerator / jnp.maximum(jnp.abs(denominator), jnp.exp(-row_max))[:, :, None]
    return (update_state(carried, key_rows, value_rows, input_gate, cumulative), output)

def memory_cell(queries, keys_in, values, input_gate, log_forget):
    length, head_count, query_width = queries.shape
    value_width = values.shape[-1]
    block_count = length // BLOCK

    def to_blocks(array, width):
        return array.astype(jnp.float32).reshape(block_count, BLOCK, head_count, width).transpose(0, 2, 1, 3)

    def gate_blocks(array):
        return array.reshape(block_count, BLOCK, head_count).transpose(0, 2, 1)
    initial = (jnp.zeros((head_count, value_width, query_width), jnp.float32), jnp.zeros((head_count, query_width), jnp.float32), jnp.zeros((head_count,), jnp.float32))
    inputs = (to_blocks(queries, query_width), to_blocks(keys_in, query_width) * query_width ** (-0.5), to_blocks(values, value_width), gate_blocks(input_gate), gate_blocks(log_forget))
    _, outputs = lax.scan(block_step, initial, inputs)
    return outputs.transpose(0, 2, 1, 3).reshape(length, head_count, value_width)

def latent_attention(queries, key_nope, key_rot, values):
    length = queries.shape[0]
    size = min(512, length)
    factor = (PLAIN_CHANNELS + ROTARY_CHANNELS) ** (-0.5)
    results = []
    for block_number in range(length // size):
        lower = block_number * size
        upper = lower + size
        query_nope = queries[lower:upper, :, :PLAIN_CHANNELS].astype(jnp.float32)
        query_rot = queries[lower:upper, :, PLAIN_CHANNELS:].astype(jnp.float32)
        scores = jnp.einsum('qhd,khd->hqk', query_nope, key_nope[:upper].astype(jnp.float32))
        scores = (scores + jnp.einsum('qhd,kd->hqk', query_rot, key_rot[:upper].astype(jnp.float32))) * factor
        allowed = jnp.arange(upper)[None, :] <= (lower + jnp.arange(size))[:, None]
        scores = jnp.where(allowed[None], scores, -jnp.inf)
        row_max = lax.optimization_barrier(jnp.max(scores, axis=-1, keepdims=True))
        probs = jnp.exp(scores - row_max)
        summed = lax.optimization_barrier(jnp.sum(probs, axis=-1))
        rounded = lax.optimization_barrier(probs.astype(jnp.bfloat16)).astype(jnp.float32)
        numerator = jnp.einsum('hqk,khd->qhd', rounded, values[:upper].astype(jnp.float32))
        results.append((numerator / summed.T[:, :, None]).astype(jnp.bfloat16))
    return jnp.concatenate(results, axis=0)

def reference(tokens, input_gain, weight_query, weight_key, weight_value, weight_outgate, weight_ingate, weight_forget, forget_shift, mem_gain, query_down_weight, latent_down_weight, down_rotary, query_gain, latent_gain, query_up_weight, key_up_weight, value_up_weight, out_memory, out_attend):
    length = tokens.shape[0]
    normed = rms_scale(tokens, input_gain).astype(jnp.bfloat16)

    def project(weight):
        return jnp.dot(normed, weight, preferred_element_type=jnp.float32)
    stored = (project(weight_query).astype(jnp.bfloat16), project(weight_key).astype(jnp.bfloat16), project(weight_value).astype(jnp.bfloat16), project(weight_outgate).astype(jnp.bfloat16))
    mem_query, mem_key, mem_value, mem_outgate = lax.optimization_barrier(stored)
    in_pre = project(weight_ingate)
    forget_pre = project(weight_forget) + forget_shift
    in_gate = SOFTCAP * jnp.tanh(in_pre / SOFTCAP)
    log_forget = jax.nn.log_sigmoid(SOFTCAP * jnp.tanh(forget_pre / SOFTCAP))
    query_latent = project(query_down_weight).astype(jnp.bfloat16)
    keyval_latent = project(latent_down_weight).astype(jnp.bfloat16)
    key_raw = project(down_rotary).astype(jnp.bfloat16)
    positions = jnp.arange(length, dtype=jnp.int32)
    cell = memory_cell(mem_query.reshape(length, MEMORY_HEADS, M_QK), mem_key.reshape(length, MEMORY_HEADS, M_QK), mem_value.reshape(length, MEMORY_HEADS, M_V), in_gate, log_forget)
    cell = cell.reshape(length, MEMORY_HEADS * M_V)
    gated = rms_scale(cell, mem_gain)
    gated = gated * jax.nn.sigmoid(mem_outgate.astype(jnp.float32))
    gated = gated.astype(jnp.bfloat16)
    normed_query = rms_scale(query_latent, query_gain).astype(jnp.bfloat16)
    normed_latent = rms_scale(keyval_latent, latent_gain).astype(jnp.bfloat16)
    query_all = jnp.dot(normed_query, query_up_weight, preferred_element_type=jnp.float32).astype(jnp.bfloat16)
    query_all = query_all.reshape(length, ATTEND_HEADS, PLAIN_CHANNELS + ROTARY_CHANNELS)
    queries = jnp.concatenate([query_all[..., :PLAIN_CHANNELS], rotate(query_all[..., PLAIN_CHANNELS:], positions)], axis=-1)
    key_nope = jnp.dot(normed_latent, key_up_weight, preferred_element_type=jnp.float32).astype(jnp.bfloat16)
    values = jnp.dot(normed_latent, value_up_weight, preferred_element_type=jnp.float32).astype(jnp.bfloat16)
    key_rot = rotate(key_raw, positions)
    attended = latent_attention(queries, key_nope.reshape(length, ATTEND_HEADS, PLAIN_CHANNELS), key_rot, values.reshape(length, ATTEND_HEADS, VALUE_CHANNELS)).reshape(length, ATTEND_HEADS * VALUE_CHANNELS)
    mem_share = MEMORY_HEADS // N_TP * M_V
    att_share = ATTEND_HEADS // N_TP * VALUE_CHANNELS
    summed = jnp.zeros((length, tokens.shape[1]), jnp.float32)
    for share in range(N_TP):
        partial_value = jnp.dot(gated[:, share * mem_share:(share + 1) * mem_share], out_memory[share * mem_share:(share + 1) * mem_share], preferred_element_type=jnp.float32)
        partial_value = partial_value + jnp.dot(attended[:, share * att_share:(share + 1) * att_share], out_attend[share * att_share:(share + 1) * att_share], preferred_element_type=jnp.float32)
        summed = summed + lax.optimization_barrier(partial_value.astype(jnp.bfloat16)).astype(jnp.float32)
    return summed.astype(jnp.bfloat16)
```

```python
import functools

import jax
import jax.numpy as jnp
from jax import lax
from jax.experimental import pallas as pl
from jax.experimental.pallas import tpu as pltpu
from jax.sharding import Mesh
from jax.sharding import PartitionSpec as P

MEMORY_HEADS = 8
M_QK = 128
M_V = 256
NOPE = 128
ROT = 64
QLAT = 768
KLAT = 512
ROWS = 512
WIDTH = 2048
EPS = 1e-06
SOFTCAP = 15.0
ROTARY_BASE = 10000.0
FAR_BELOW = -1e30
LOG2E = 1.4426950408889634
F32 = jnp.float32
BF16 = jnp.bfloat16
NZ, NX, NY, NC = 8, 4, 4, 2


def dot(a, b, dims=((1,), (0,))):
    return lax.dot_general(a, b, (dims, ((), ())), preferred_element_type=F32)


def split2(a):
    hi = a.astype(BF16)
    return hi, (a - hi.astype(F32)).astype(BF16)


def split3(a):
    hi = a.astype(BF16)
    rest = a - hi.astype(F32)
    mid = rest.astype(BF16)
    return hi, mid, (rest - mid.astype(F32)).astype(BF16)


def vmem():
    return pl.BlockSpec(memory_space=pltpu.VMEM)


def smem():
    return pl.BlockSpec(memory_space=pltpu.SMEM)


def kernel(body, outs, name, n_in, scratch=(), flops=0, scalars=True, aliases=None):
    specs = ([smem()] if scalars else []) + [vmem()] * n_in
    return pl.pallas_call(
        body,
        out_shape=outs,
        in_specs=specs,
        out_specs=jax.tree.map(lambda _: vmem(), outs),
        scratch_shapes=list(scratch),
        name=name,
        input_output_aliases=aliases or {},
        compiler_params=pltpu.CompilerParams(vmem_limit_bytes=48 * 1024 * 1024),
        cost_estimate=pl.CostEstimate(flops=flops, bytes_accessed=0, transcendentals=0),
    )


def sds(shape, dtype):
    return jax.ShapeDtypeStruct(shape, dtype)


def norm_body(tokens, gain, out):
    t = tokens[...].astype(F32)
    scale = lax.rsqrt(jnp.mean(t * t, axis=-1, keepdims=True) + EPS)
    out[...] = (t * scale * gain[...].astype(F32)).astype(BF16)


def latent_body(pos, *refs):
    pieces, (w, x_out, rot_out, lat_out) = refs[:8], refs[8:]
    y, c = pos[2], pos[3]
    for k in range(NY):
        yy = lax.rem(y + NY - k, NY)
        for side in range(NC):
            cc = c if side == 0 else 1 - c
            at = pl.multiple_of((2 * yy + cc) * 64, 64)
            x_out[pl.ds(at, 64), :] = pieces[2 * k + side][...]
    lat = dot(x_out[...], w[...])
    lat_t = lat.T
    rot_out[...] = lat_t[0:ROT].astype(BF16)
    lat_out[...] = lat_t[ROT : ROT + 160].astype(BF16)


def memory_body(pos, x_ref, wqk, wvo, wg, shift, q_out, k_out, v_out, og_out, gates_out, s0, s1, s2, s3, c_scr):
    xx = x_ref[...]
    pre = dot(wg[...], xx, ((1,), (1,)))
    in_gate = SOFTCAP * jnp.tanh(pre[0:1] / SOFTCAP)
    f = SOFTCAP * jnp.tanh((pre[1:2] + shift[...]) / SOFTCAP)
    log_forget = jnp.minimum(f, 0.0) - jnp.log1p(jnp.exp(-jnp.abs(f)))
    row = lax.broadcasted_iota(jnp.int32, (ROWS, ROWS), 0)
    col = lax.broadcasted_iota(jnp.int32, (ROWS, ROWS), 1)
    upper = (row <= col).astype(BF16)
    parts = split3(jnp.broadcast_to(log_forget, (16, ROWS)))
    cum = (dot(parts[0], upper) + dot(parts[1], upper) + dot(parts[2], upper))[0:1]
    pack = jnp.concatenate([cum, in_gate, jnp.zeros((6, ROWS), F32)], axis=0)
    gates_out[...] = pack
    cols = pack.T
    total = cum[:, ROWS - 1 : ROWS]
    weight = jnp.exp(total - cols[:, 0:1] + cols[:, 1:2])
    qk = dot(xx, wqk[...])
    q_out[...] = qk[:, :M_QK].astype(BF16)
    k = qk[:, M_QK:].astype(BF16)
    k_out[...] = k
    vo = dot(xx, wvo[...])
    v = vo[:, :M_V].astype(BF16)
    v_out[...] = v
    og_out[...] = vo[:, M_V:].astype(BF16)
    kw = k.astype(F32) * (M_QK**-0.5) * weight
    a, b, e = split3(kw)
    zero = ((0,), (0,))
    c_scr[...] = dot(v, a, zero) + dot(v, b, zero) + dot(v, e, zero)
    normal = jnp.sum(kw, axis=0, keepdims=True)
    tail = jnp.concatenate(
        [normal, jnp.broadcast_to(total, (1, M_QK)), jnp.zeros((6, M_QK), F32)], axis=0
    )
    for d, ref in enumerate((s0, s1, s2, s3)):
        at = pl.multiple_of(lax.rem(pos[1] + d, NX) * 64, 64)
        ref[0:64, :] = c_scr[pl.ds(at, 64), :]
        ref[64:72, :] = tail


def group_body(pos, r0, r1, r2, r3, group_out, inside_out, scr):
    for d, ref in enumerate((r0, r1, r2, r3)):
        scr[lax.rem(pos[1] + NX - d, NX)] = ref[...]
    run = jnp.zeros((72, M_QK), F32)
    logs = jnp.zeros((1, M_QK), F32)
    row = lax.broadcasted_iota(jnp.int32, (72, M_QK), 0)
    for k in range(NX):
        inside_out[k] = jnp.where(row == 65, logs, run)
        step = scr[k]
        run = jnp.exp(step[65:66]) * run + step
        logs = logs + step[65:66]
    group_out[...] = jnp.where(row == 65, logs, run)


def carry_body(pos, inside, g1, g2, g3, g4, g5, g6, g7, o0, o1, o2, o3):
    run = jnp.zeros((72, M_QK), F32)
    for g in (g7, g6, g5, g4, g3, g2, g1):
        step = g[...]
        run = jnp.exp(step[65:66]) * run + step
    for d, ref in enumerate((o0, o1, o2, o3)):
        mine = inside[lax.rem(pos[1] + d, NX)]
        ref[...] = jnp.exp(mine[65:66]) * run + mine


def cell_body(pos, q_ref, k_ref, v_ref, gates, r0, r1, r2, r3, cell_out, ss_out, c_scr):
    for d, ref in enumerate((r0, r1, r2, r3)):
        at = pl.multiple_of(lax.rem(pos[1] + NX - d, NX) * 64, 64)
        c_scr[pl.ds(at, 64), :] = ref[0:64, :]
    normal = r0[64:65, :]
    state = c_scr[...]
    c3 = split3(state)
    pack = gates[...]
    cum_row = pack[0:1]
    in_row = pack[1:2]
    cols = pack.T
    size = 128
    for t in range(ROWS // size):
        lo, hi = t * size, (t + 1) * size
        qt = q_ref[lo:hi, :]
        cum_col = cols[lo:hi, 0:1]
        scores = dot(qt, k_ref[0:hi, :], ((1,), (1,))) * (M_QK**-0.5)
        logw = cum_col - cum_row[:, 0:hi] + in_row[:, 0:hi]
        row = lax.broadcasted_iota(jnp.int32, (size, hi), 0) + lo
        col = lax.broadcasted_iota(jnp.int32, (size, hi), 1)
        weights = jnp.exp(jnp.where(col <= row, logw, FAR_BELOW))
        aff = scores * weights
        across = jnp.exp(cum_col)
        den = jnp.sum(aff, axis=1, keepdims=True) + across * jnp.sum(
            qt.astype(F32) * normal, axis=1, keepdims=True
        )
        a, b = split2(aff)
        vv = v_ref[0:hi, :]
        num = dot(a, vv) + dot(b, vv)
        nt = ((1,), (1,))
        inter = dot(qt, c3[0], nt) + dot(qt, c3[1], nt) + dot(qt, c3[2], nt)
        cell = (num + across * inter) / jnp.maximum(jnp.abs(den), 1.0)
        cell_out[lo:hi, :] = cell
        ss = jnp.sum(cell * cell, axis=1, keepdims=True)
        ss_out[:, lo:hi] = jnp.broadcast_to(ss, (size, 128)).T[0:8]


def gate_body(cell, t0, t1, t2, t3, gain, og, out):
    total = t0[...] + t1[...] + t2[...] + t3[...]
    scale = lax.rsqrt(total / (MEMORY_HEADS * M_V) + EPS)
    col = scale.T[:, 0:1]
    gated = cell[...] * col * gain[...]
    out[...] = (gated * jax.nn.sigmoid(og[...].astype(F32))).astype(BF16)


def up_body(pos, *refs):
    pieces = refs[:8]
    rot_raw, wq, wkv, qgain, kgain, cos, sin, q_out, kv_out, ql, kl = refs[8:]
    y, c = pos[2], pos[3]
    for k in range(NY):
        yy = lax.rem(y + NY - k, NY)
        for side in range(NC):
            cc = c if side == 0 else 1 - c
            index = 2 * yy + cc
            piece = pieces[2 * k + side]
            ql[pl.ds(pl.multiple_of(index * 96, 32), 96), :] = piece[0:96, :]
            kl[pl.ds(pl.multiple_of(index * 64, 64), 64), :] = piece[96:160, :]

    def turn(u):
        u1, u2 = u[0:32], u[32:64]
        cc, ss = cos[...], sin[...]
        return jnp.concatenate([u1 * cc - u2 * ss, u2 * cc + u1 * ss], axis=0)

    kf = kl[...].astype(F32)
    nk = kf * lax.rsqrt(jnp.mean(kf * kf, axis=0, keepdims=True) + EPS) * kgain[...]
    kv = dot(wkv[...], nk.astype(BF16))
    key_rot = turn(rot_raw[...].astype(F32))
    keys = jnp.concatenate([kv[0:NOPE], key_rot, jnp.zeros((64, ROWS), F32)], axis=0).T
    kv_out[0:512, :] = keys[:, 0:NOPE].astype(BF16)
    rot = keys[:, NOPE:]
    kv_out[512:768, :] = (rot[0:256] + pltpu.roll(rot[256:512], 64, 1)).astype(BF16)
    for i in range(4):
        kv_out[768 + 128 * i : 896 + 128 * i, :] = kv[NOPE:, 128 * i : 128 * (i + 1)].astype(BF16)
    qf = ql[...].astype(F32)
    nq = qf * lax.rsqrt(jnp.mean(qf * qf, axis=0, keepdims=True) + EPS) * qgain[...]
    qt = dot(wq[...], nq.astype(BF16)).astype(BF16)
    q_out[0:NOPE, :] = qt[0:NOPE]
    q_out[NOPE:, :] = turn(qt[NOPE:].astype(F32)).astype(BF16)


DOWN = {1: (7, 0, 1), 2: (7, 6, 0), 3: (7, 6, 5)}
FACTOR = (NOPE + ROT) ** -0.5 * LOG2E
TILE = 256


def attend_tile(q_ref, kv, acc, ml, d, causal):
    zeros = jnp.zeros((64, TILE), BF16)
    for h in range(ROWS // TILE):
        lo, hi = h * TILE, (h + 1) * TILE
        keys_hi = hi if causal else ROWS
        nope = q_ref[0:NOPE, lo:hi]
        turned = q_ref[NOPE:, lo:hi]
        rotp = kv[512:768, :]
        parts = []
        for part in range(keys_hi // 256):
            side = [turned, zeros] if part == 0 else [zeros, turned]
            qq = jnp.concatenate([nope] + side, axis=0)
            kk = jnp.concatenate([kv[256 * part : 256 * (part + 1), :], rotp], axis=1)
            s = dot(kk, qq) * FACTOR
            if causal and part == h:
                key = lax.broadcasted_iota(jnp.int32, (256, TILE), 0)
                qry = lax.broadcasted_iota(jnp.int32, (256, TILE), 1)
                s = jnp.where(key <= qry, s, FAR_BELOW)
            parts.append(s)
        at = slice(d * ROWS + lo, d * ROWS + hi)
        old = ml[0:1, at]
        new = old
        for s in parts:
            new = jnp.maximum(new, jnp.max(s, axis=0, keepdims=True))
        shrink = jnp.exp2(old - new)
        total = ml[1:2, at] * shrink
        value = acc[:, at] * shrink
        for part, s in enumerate(parts):
            p = jnp.exp2(s - new)
            total = total + jnp.sum(p, axis=0, keepdims=True)
            base = 768 + 256 * part
            vt = jnp.concatenate([kv[base : base + 128, :], kv[base + 128 : base + 256, :]], axis=1)
            value = value + dot(vt, p.astype(BF16))
        ml[0:1, at] = new
        ml[1:2, at] = total
        acc[:, at] = value


def own_body(pos, q0, q1, q2, q3, kv, acc, ml):
    acc[...] = jnp.zeros(acc.shape, F32)
    ml[0:1, :] = jnp.full((1, 4 * ROWS), FAR_BELOW, F32)
    ml[1:8, :] = jnp.zeros((7, 4 * ROWS), F32)
    attend_tile(q0, kv, acc, ml, 0, True)
    for d, q in ((1, q1), (2, q2), (3, q3)):

        @pl.when(pos[1] < d)
        def _(q=q, d=d):
            attend_tile(q, kv, acc, ml, d, False)


def ring_body(up_step, down_step, final, pos, *refs):
    qs = refs[:4]
    n = (up_step > 0) + (down_step > 0)
    chunks = refs[4 : 4 + n]
    acc_in, ml_in = refs[4 + n : 6 + n]
    outs = refs[6 + n :]
    if final:
        packets, (acc, ml) = outs[:4], outs[4:]
    else:
        acc, ml = outs
    acc[...] = acc_in[...]
    ml[...] = ml_in[...]
    conditions = []
    if up_step:
        conditions.append(pos[0] >= up_step)
    if down_step:
        conditions.append(pos[0] + down_step >= NZ)
    for cond, chunk in zip(conditions, chunks):

        @pl.when(cond)
        def _(chunk=chunk):
            for d in range(4):
                attend_tile(qs[d], chunk, acc, ml, d, False)

    if final:
        for d in range(4):
            at = slice(d * ROWS, (d + 1) * ROWS)
            total = jnp.maximum(ml[1:2, at], 1e-30)
            packets[d][0:128, :] = (acc[:, at] / total).astype(BF16)
            a, b, e = split3(ml[0:1, at] + jnp.log2(total))
            packets[d][128:144, :] = jnp.concatenate([a, b, e, jnp.zeros((13, ROWS), BF16)], axis=0)


def out_body(pos, p0, p1, p2, p3, gated, wmem, watt, k0, k1, k2, k3, n0, n1, n2, n3, scr):
    packets = (p0, p1, p2, p3)
    logs = []
    for p in packets:
        s = p[128:144, :].astype(F32)
        logs.append(s[0:1] + s[1:2] + s[2:3])
    top = jnp.maximum(jnp.maximum(logs[0], logs[1]), jnp.maximum(logs[2], logs[3]))
    weights = [jnp.exp2(v - top) for v in logs]
    total = weights[0] + weights[1] + weights[2] + weights[3]
    att = jnp.zeros((128, ROWS), F32)
    for p, w in zip(packets, weights):
        att = att + p[0:128, :].astype(F32) * (w / total)
    att = att.T.astype(BF16)
    scr[...] = (dot(gated[...], wmem[...]) + dot(att, watt[...])).astype(BF16)
    y, c = pos[2], pos[3]
    for d, (keep, send) in enumerate(zip((k0, k1, k2, k3), (n0, n1, n2, n3))):
        yy = lax.rem(y + d, NY)
        keep[...] = scr[pl.ds(pl.multiple_of((2 * yy + c) * 64, 64), 64), :]
        send[...] = scr[pl.ds(pl.multiple_of((2 * yy + 1 - c) * 64, 64), 64), :]


def shift(a, axis, size, by):
    return lax.ppermute(a, axis, [(i, (i + by) % size) for i in range(size)])


def swap(a):
    return shift(a, "c", NC, 1)


def over_tp(piece):
    near = [piece] + [shift(piece, "y", NY, k) for k in (1, 2, 3)]
    pieces = []
    for p in near:
        pieces += [p, swap(p)]
    return pieces


def per_device(
    tokens,
    input_gain,
    weight_query,
    weight_key,
    weight_value,
    weight_outgate,
    weight_ingate,
    weight_forget,
    forget_shift,
    mem_gain,
    query_down_weight,
    latent_down_weight,
    down_rotary,
    query_gain,
    latent_gain,
    query_up_weight,
    key_up_weight,
    value_up_weight,
    out_memory,
    out_attend,
):
    zi, xi = lax.axis_index("z"), lax.axis_index("x")
    yi, ci = lax.axis_index("y"), lax.axis_index("c")
    tp = yi * NC + ci
    pos = jnp.stack([zi, xi, yi, ci]).astype(jnp.int32)

    normed = kernel(norm_body, sds((64, WIDTH), BF16), "norm", 2, scalars=False)(
        tokens, input_gain.reshape(1, WIDTH)
    )

    w_lat = jnp.concatenate(
        [down_rotary, query_down_weight, latent_down_weight, jnp.zeros((WIDTH, 32), BF16)], axis=1
    )
    w_qk = jnp.concatenate([weight_query, weight_key], axis=1)
    w_vo = jnp.concatenate([weight_value, weight_outgate], axis=1)
    w_gates = jnp.concatenate(
        [
            lax.dynamic_slice_in_dim(weight_ingate, tp, 1, 1).T,
            lax.dynamic_slice_in_dim(weight_forget, tp, 1, 1).T,
            jnp.zeros((14, WIDTH), BF16),
        ],
        axis=0,
    )
    w_qup = query_up_weight.T
    w_kvup = jnp.concatenate([key_up_weight, value_up_weight], axis=1).T
    gain_part = lax.dynamic_slice_in_dim(mem_gain, tp * M_V, M_V, 0).astype(F32).reshape(1, M_V)
    shift_row = forget_shift.reshape(1, ROWS)
    qgain, kgain = query_gain.reshape(QLAT, 1), latent_gain.reshape(KLAT, 1)
    positions = (zi * NX + xi) * ROWS + jnp.arange(ROWS, dtype=jnp.int32)
    inverse = jnp.power(ROTARY_BASE, -jnp.arange(32, dtype=F32) / 32)
    angles = positions.astype(F32)[None, :] * inverse[:, None]
    cos, sin = jnp.cos(angles), jnp.sin(angles)

    pieces = over_tp(normed)
    x_all, rot_raw, latents = kernel(
        latent_body,
        (sds((ROWS, WIDTH), BF16), sds((ROT, ROWS), BF16), sds((160, ROWS), BF16)),
        "latents",
        9,
        flops=2 * ROWS * WIDTH * 512,
    )(pos, *pieces, w_lat)

    lat_pieces = over_tp(latents)

    quarter = sds((72, M_QK), F32)
    q, k, v, og, gates, *states = kernel(
        memory_body,
        (
            sds((ROWS, M_QK), BF16),
            sds((ROWS, M_QK), BF16),
            sds((ROWS, M_V), BF16),
            sds((ROWS, M_V), BF16),
            sds((8, ROWS), F32),
            quarter,
            quarter,
            quarter,
            quarter,
        ),
        "memory",
        5,
        scratch=[pltpu.VMEM((M_V, M_QK), F32)],
        flops=2 * ROWS * WIDTH * 1600,
    )(pos, x_all, w_qk, w_vo, w_gates, shift_row)
    arrived = [states[0]] + [shift(states[d], "x", NX, d) for d in (1, 2, 3)]

    q_t, kv0 = kernel(
        up_body,
        (sds((192, ROWS), BF16), sds((1280, 128), BF16)),
        "up",
        15,
        scratch=[pltpu.VMEM((QLAT, ROWS), BF16), pltpu.VMEM((KLAT, ROWS), BF16)],
        flops=2 * ROWS * WIDTH * 700,
    )(pos, *lat_pieces, rot_raw, w_qup, w_kvup, qgain, kgain, cos, sin)

    up, down = [kv0], [kv0]
    for t in range(1, 5):
        up.append(lax.ppermute(up[-1], "z", [(i, i + 1) for i in range(t - 1, NZ - 1)]))
        if t < 4:
            down.append(lax.ppermute(down[-1], "z", [((j + 1) % NZ, j) for j in DOWN[t]]))
    qs = [q_t] + [shift(q_t, "x", NX, d) for d in (1, 2, 3)]

    group, inside = kernel(
        group_body,
        (quarter, sds((NX, 72, M_QK), F32)),
        "group",
        4,
        scratch=[pltpu.VMEM((NX, 72, M_QK), F32)],
        flops=2 * 10**8,
    )(pos, *arrived)
    before = [lax.ppermute(group, "z", [(i, i + d) for i in range(NZ - d)]) for d in range(1, NZ)]
    carried = kernel(carry_body, (quarter,) * 4, "carry", 8, flops=2 * 10**8)(pos, inside, *before)
    entered = [carried[0]] + [shift(carried[d], "x", NX, d) for d in (1, 2, 3)]
    cell, ss = kernel(
        cell_body,
        (sds((ROWS, M_V), F32), sds((8, ROWS), F32)),
        "cell",
        8,
        scratch=[pltpu.VMEM((M_V, M_QK), F32)],
        flops=2 * ROWS * WIDTH * 1600,
    )(pos, q, k, v, gates, *entered)
    ss = ss + swap(ss)
    sums = [ss] + [shift(ss, "y", NY, d) for d in (1, 2, 3)]
    gated = kernel(gate_body, sds((ROWS, M_V), BF16), "gate", 7, scalars=False, flops=10**9)(
        cell, *sums, gain_part, og
    )

    state = (sds((128, 4 * ROWS), F32), sds((8, 4 * ROWS), F32))
    tile_flops = 4 * 2 * ROWS * ROWS * 384
    acc, ml = kernel(own_body, state, "own", 5, flops=tile_flops)(pos, *qs, kv0)
    packet = sds((144, ROWS), BF16)
    for t in range(1, 5):
        last = t == 4
        chunks = [up[t]] + ([] if last else [down[t]])
        n = len(chunks)
        res = kernel(
            functools.partial(ring_body, t, 0 if last else t, last),
            (packet,) * 4 if last else state,
            f"ring{t}",
            6 + n,
            flops=tile_flops * n,
            scratch=[pltpu.VMEM(s.shape, s.dtype) for s in state] if last else (),
            aliases=None if last else {5 + n: 0, 6 + n: 1},
        )(pos, *qs, *chunks, acc, ml)
        if last:
            packets = res
        else:
            acc, ml = res

    back = [packets[0]] + [shift(packets[d], "x", NX, -d) for d in (1, 2, 3)]
    block = sds((64, WIDTH), BF16)
    res = kernel(
        out_body,
        (block,) * 8,
        "out",
        7,
        scratch=[pltpu.VMEM((ROWS, WIDTH), BF16)],
        flops=2 * ROWS * WIDTH * 600,
    )(pos, *back, gated, out_memory, out_attend)
    keep, send = res[:4], res[4:]
    got = [swap(s) for s in send]
    pair = [a.astype(F32) + b.astype(F32) for a, b in zip(keep, got)]
    total = pair[0]
    for d in (2, 1, 3):
        total = total + shift(pair[d].astype(BF16), "y", NY, d).astype(F32)
    return total.astype(BF16)


def solution(mesh):
    torus = Mesh(mesh.devices.reshape(NZ, NX, NY, NC), ("z", "x", "y", "c"))
    sp, tp = ("z", "x"), ("y", "c")
    rows = P(("z", "x", "y", "c"), None)
    in_specs = (
        rows,
        P(),
        P(None, tp),
        P(None, tp),
        P(None, tp),
        P(None, tp),
        P(),
        P(),
        P(sp, tp),
        P(),
        P(None, tp),
        P(None, tp),
        P(),
        P(),
        P(),
        P(None, tp),
        P(None, tp),
        P(None, tp),
        P(tp, None),
        P(tp, None),
    )
    return jax.shard_map(
        per_device, mesh=torus, in_specs=in_specs, out_specs=rows, check_vma=False
    )
```

```python
import functools

import jax
import jax.numpy as jnp
from jax import lax
from jax.experimental import pallas as pl
from jax.experimental.pallas import tpu as pltpu
from jax.sharding import Mesh
from jax.sharding import PartitionSpec as P

MEMORY_HEADS = 8
M_QK = 128
M_V = 256
NOPE = 128
ROT = 64
QLAT = 768
KLAT = 512
ROWS = 512
WIDTH = 2048
EPS = 1e-06
SOFTCAP = 15.0
ROTARY_BASE = 10000.0
FAR_BELOW = -1e30
LOG2E = 1.4426950408889634
F32 = jnp.float32
BF16 = jnp.bfloat16
NZ, NX, NY, NC = 8, 4, 4, 2


def dot(a, b, dims=((1,), (0,))):
    return lax.dot_general(a, b, (dims, ((), ())), preferred_element_type=F32)


def split2(a):
    hi = a.astype(BF16)
    return hi, (a - hi.astype(F32)).astype(BF16)


def split3(a):
    hi = a.astype(BF16)
    rest = a - hi.astype(F32)
    mid = rest.astype(BF16)
    return hi, mid, (rest - mid.astype(F32)).astype(BF16)


def vmem():
    return pl.BlockSpec(memory_space=pltpu.VMEM)


def smem():
    return pl.BlockSpec(memory_space=pltpu.SMEM)


def kernel(body, outs, n_in, scratch=(), flops=0, scalars=True, aliases=None, far=0):
    specs = ([smem()] if scalars else []) + [vmem()] * (n_in - far)
    specs += [pl.BlockSpec(memory_space=pltpu.HBM)] * far
    return pl.pallas_call(
        body,
        out_shape=outs,
        in_specs=specs,
        out_specs=jax.tree.map(lambda _: vmem(), outs),
        scratch_shapes=list(scratch),
        input_output_aliases=aliases or {},
        compiler_params=pltpu.CompilerParams(vmem_limit_bytes=20 * 1024 * 1024),
        cost_estimate=pl.CostEstimate(flops=flops, bytes_accessed=0, transcendentals=0),
    )


def sds(shape, dtype):
    return jax.ShapeDtypeStruct(shape, dtype)


def norm_body(tokens, gain, out):
    t = tokens[...].astype(F32)
    scale = lax.rsqrt(jnp.mean(t * t, axis=-1, keepdims=True) + EPS)
    out[...] = (t * scale * gain[...].astype(F32)).astype(BF16)


def latent_body(pos, *refs):
    pieces, (w_rot, w_q, w_k, x_out, rot_out, lat_out, w, sems) = refs[:8], refs[8:]
    ends = ((w_rot, 0, 64), (w_q, 64, 160), (w_k, 160, 224))
    loads = [
        pltpu.make_async_copy(src, w.at[lo:hi, :], sems.at[i])
        for i, (src, lo, hi) in enumerate(ends)
    ]
    for load in loads:
        load.start()
    y, c = pos[2], pos[3]
    for k in range(NY):
        yy = lax.rem(y + NY - k, NY)
        for side in range(NC):
            cc = c if side == 0 else 1 - c
            at = pl.multiple_of((2 * yy + cc) * 64, 64)
            x_out[pl.ds(at, 64), :] = pieces[2 * k + side][...]
    for load in loads:
        load.wait()
    lat_t = dot(w[...], x_out[...], ((1,), (1,)))
    rot_out[...] = lat_t[0:ROT].astype(BF16)
    lat_out[...] = lat_t[ROT : ROT + 160].astype(BF16)


def memory_body(pos, x_ref, wq, wk, wv, wo, wg, shift, q_out, k_out, v_out, og_out, gates_out, s0, s1, s2, s3, c_scr):
    xx = x_ref[...]
    pre = dot(wg[...], xx, ((1,), (1,)))
    in_gate = SOFTCAP * jnp.tanh(pre[0:1] / SOFTCAP)
    f = SOFTCAP * jnp.tanh((pre[1:2] + shift[...]) / SOFTCAP)
    log_forget = jnp.minimum(f, 0.0) - jnp.log1p(jnp.exp(-jnp.abs(f)))
    row = lax.broadcasted_iota(jnp.int32, (ROWS, ROWS), 0)
    col = lax.broadcasted_iota(jnp.int32, (ROWS, ROWS), 1)
    upper = (row <= col).astype(BF16)
    parts = split3(jnp.broadcast_to(log_forget, (16, ROWS)))
    cum = (dot(parts[0], upper) + dot(parts[1], upper) + dot(parts[2], upper))[0:1]
    pack = jnp.concatenate([cum, in_gate, jnp.zeros((6, ROWS), F32)], axis=0)
    gates_out[...] = pack
    cols = pack.T
    total = cum[:, ROWS - 1 : ROWS]
    weight = jnp.exp(total - cols[:, 0:1] + cols[:, 1:2])
    qk = dot(xx, jnp.concatenate([wq[...], wk[...]], axis=1))
    q_out[...] = qk[:, :M_QK].astype(BF16)
    k = qk[:, M_QK:].astype(BF16)
    k_out[...] = k
    v = dot(xx, wv[...]).astype(BF16)
    v_out[...] = v
    og_out[...] = dot(xx, wo[...]).astype(BF16)
    kw = k.astype(F32) * (M_QK**-0.5) * weight
    a, b, e = split3(kw)
    zero = ((0,), (0,))
    c_scr[...] = dot(v, a, zero) + dot(v, b, zero) + dot(v, e, zero)
    normal = jnp.sum(kw, axis=0, keepdims=True)
    tail = jnp.concatenate(
        [normal, jnp.broadcast_to(total, (1, M_QK)), jnp.zeros((6, M_QK), F32)], axis=0
    )
    for d, ref in enumerate((s0, s1, s2, s3)):
        at = pl.multiple_of(lax.rem(pos[1] + d, NX) * 64, 64)
        ref[0:64, :] = c_scr[pl.ds(at, 64), :]
        ref[64:72, :] = tail


def pack_state(ref):
    hi, mid = split2(ref[0:64, :])
    body = jnp.concatenate([hi[0:32], hi[32:64], mid[0:32], mid[32:64]], axis=1)
    a, b, e = split3(ref[64:72, :])
    tail = jnp.concatenate([a, b, e, jnp.zeros((8, 128), BF16)], axis=1)
    return jnp.concatenate([body, tail, jnp.zeros((8, 512), BF16)], axis=0)


def unpack_state(ref):
    f = ref[192:240, :].astype(F32)
    top = f[0:32, 0:128] + f[0:32, 256:384]
    low = f[0:32, 128:256] + f[0:32, 384:512]
    tail = f[32:40, 0:128] + f[32:40, 128:256] + f[32:40, 256:384]
    return jnp.concatenate([top, low, tail], axis=0)


def chain(earlier, later):
    row = lax.broadcasted_iota(jnp.int32, (72, M_QK), 0)
    return jnp.where(row == 65, earlier, jnp.exp(later[65:66]) * earlier) + later


def group_body(pos, r0, r1, r2, r3, group_out, inside_out, scr):
    for d, ref in enumerate((r0, r1, r2, r3)):
        scr[lax.rem(pos[1] + NX - d, NX)] = unpack_state(ref)
    run = jnp.zeros((72, M_QK), F32)
    for k in range(NX):
        inside_out[k] = run
        run = chain(run, scr[k])
    group_out[...] = run


def scan_one_body(before, group, window_out):
    window_out[...] = chain(before[...], group[...])


def scan_two_body(before, window, entry, window_out, entry_out):
    window_out[...] = chain(before[...], window[...])
    entry_out[...] = chain(before[...], entry[...])


def carry_body(pos, inside, before, entry, o0, o1, o2, o3):
    run = chain(before[...], entry[...])
    for d, ref in enumerate((o0, o1, o2, o3)):
        ref[...] = chain(run, inside[lax.rem(pos[1] + d, NX)])


def cell_body(pos, q_ref, k_ref, v_ref, gates, r0, r1, r2, r3, cell_out, ss_out, c_scr):
    for d, ref in enumerate((r0, r1, r2, r3)):
        at = pl.multiple_of(lax.rem(pos[1] + NX - d, NX) * 64, 64)
        c_scr[pl.ds(at, 64), :] = ref[0:64, :]
    normal = r0[64:65, :]
    state = c_scr[...]
    c3 = split3(state)
    pack = gates[...]
    cum_row = pack[0:1]
    in_row = pack[1:2]
    cols = pack.T
    size = 128
    for t in range(ROWS // size):
        lo, hi = t * size, (t + 1) * size
        qt = q_ref[lo:hi, :]
        cum_col = cols[lo:hi, 0:1]
        scores = dot(qt, k_ref[0:hi, :], ((1,), (1,))) * (M_QK**-0.5)
        logw = cum_col - cum_row[:, 0:hi] + in_row[:, 0:hi]
        row = lax.broadcasted_iota(jnp.int32, (size, hi), 0) + lo
        col = lax.broadcasted_iota(jnp.int32, (size, hi), 1)
        weights = jnp.exp(jnp.where(col <= row, logw, FAR_BELOW))
        aff = scores * weights
        across = jnp.exp(cum_col)
        den = jnp.sum(aff, axis=1, keepdims=True) + across * jnp.sum(
            qt.astype(F32) * normal, axis=1, keepdims=True
        )
        a, b = split2(aff)
        vv = v_ref[0:hi, :]
        num = dot(a, vv) + dot(b, vv)
        nt = ((1,), (1,))
        inter = dot(qt, c3[0], nt) + dot(qt, c3[1], nt) + dot(qt, c3[2], nt)
        cell = (num + across * inter) / jnp.maximum(jnp.abs(den), 1.0)
        cell_out[lo:hi, :] = cell
        ss = jnp.sum(cell * cell, axis=1, keepdims=True)
        ss_out[:, lo:hi] = jnp.broadcast_to(ss, (size, 128)).T[0:8]


def gate_body(cell, t0, t1, t2, t3, gain, og, out):
    total = t0[...] + t1[...] + t2[...] + t3[...]
    scale = lax.rsqrt(total / (MEMORY_HEADS * M_V) + EPS)
    col = scale.T[:, 0:1]
    gated = cell[...] * col * gain[...]
    out[...] = (gated * jax.nn.sigmoid(og[...].astype(F32))).astype(BF16)


def as_column(ref):
    return jnp.broadcast_to(ref[...], (8, ref.shape[1])).T[:, 0:1]


def up_body(pos, *refs):
    pieces = refs[:8]
    rot_raw, wq, wk, wv, qgain, kgain, cos, sin = refs[8:16]
    states, packets, (kv_out, ql, kl) = refs[16:20], refs[20:24], refs[24:]
    y, c = pos[2], pos[3]
    for k in range(NY):
        yy = lax.rem(y + NY - k, NY)
        for side in range(NC):
            cc = c if side == 0 else 1 - c
            index = 2 * yy + cc
            piece = pieces[2 * k + side]
            ql[pl.ds(pl.multiple_of(index * 96, 32), 96), :] = piece[0:96, :]
            kl[pl.ds(pl.multiple_of(index * 64, 64), 64), :] = piece[96:160, :]

    def turn(u):
        u1, u2 = u[0:32], u[32:64]
        cc, ss = cos[...], sin[...]
        return jnp.concatenate([u1 * cc - u2 * ss, u2 * cc + u1 * ss], axis=0)

    kf = kl[...].astype(F32)
    nk = kf * lax.rsqrt(jnp.mean(kf * kf, axis=0, keepdims=True) + EPS) * as_column(kgain)
    kv = dot(jnp.concatenate([wk[...], wv[...]], axis=1), nk.astype(BF16), ((0,), (0,)))
    key_rot = turn(rot_raw[...].astype(F32))
    keys = jnp.concatenate([kv[0:NOPE], key_rot, jnp.zeros((64, ROWS), F32)], axis=0).T
    kv_out[0:512, :] = keys[:, 0:NOPE].astype(BF16)
    rot = keys[:, NOPE:]
    kv_out[512:768, :] = (rot[0:256] + pltpu.roll(rot[256:512], 64, 1)).astype(BF16)
    for i in range(4):
        kv_out[768 + 128 * i : 896 + 128 * i, :] = kv[NOPE:, 128 * i : 128 * (i + 1)].astype(BF16)
    qf = ql[...].astype(F32)
    nq = qf * lax.rsqrt(jnp.mean(qf * qf, axis=0, keepdims=True) + EPS) * as_column(qgain)
    qt = dot(wq[...], nq.astype(BF16)).astype(BF16)
    turned = turn(qt[NOPE:].astype(F32)).astype(BF16)
    for packet, state in zip(packets, states):
        packet[0:NOPE, :] = qt[0:NOPE]
        packet[NOPE : NOPE + ROT, :] = turned
        packet[192:240, :] = pack_state(state)


DOWN = {1: (7, 0, 1), 2: (7, 6, 0), 3: (7, 6, 5)}
FACTOR = (NOPE + ROT) ** -0.5 * LOG2E


def spread_keys(kv, kk):
    kk[:, 0:NOPE] = kv[0:512, :]
    rot = kv[512:768, :].astype(F32)
    lane = lax.broadcasted_iota(jnp.int32, (256, 128), 1)
    kk[0:256, NOPE:] = jnp.where(lane < ROT, rot, 0.0).astype(BF16)
    kk[256:512, NOPE:] = jnp.where(lane < ROT, pltpu.roll(rot, 64, 1), 0.0).astype(BF16)


def diagonal(q, kk, vt, acc, m, l):
    for h in range(2):
        lo, hi = h * 256, (h + 1) * 256
        s = dot(kk[0:hi, :], q[:, lo:hi]) * FACTOR
        key = lax.broadcasted_iota(jnp.int32, (hi, 256), 0)
        qry = lax.broadcasted_iota(jnp.int32, (hi, 256), 1) + lo
        s = jnp.where(key <= qry, s, FAR_BELOW)
        new = jnp.max(s, axis=0, keepdims=True)
        p = jnp.exp2(s - new)
        m[0:1, lo:hi] = new
        l[0:1, lo:hi] = jnp.sum(p, axis=0, keepdims=True)
        acc[:, lo:hi] = dot(vt[:, 0:hi], p.astype(BF16))


def attend(count, qall, kk, vt, acc, m, l, bufs):
    (s_a, w_a, p_a, h_a), (s_b, w_b, p_b, h_b) = bufs

    def place(i):
        d = lax.rem(i, NX)
        return d, pl.ds(pl.multiple_of(d * ROWS, ROWS), ROWS), lax.div(i, NX)

    def scores(i, s_ref, w_ref):
        d, at, chunk = place(i)
        s = dot(kk[chunk], qall[d]) * FACTOR
        old = m[0:1, at]
        new = jnp.maximum(old, jnp.max(s, axis=0, keepdims=True))
        s_ref[...] = s
        w_ref[0:1, :] = new
        w_ref[1:2, :] = jnp.exp2(old - new)
        m[0:1, at] = new

    def probs(i, s_ref, w_ref, p_ref, h_ref):
        _, at, _ = place(i)
        p = jnp.exp2(s_ref[...] - w_ref[0:1, :])
        shrink = w_ref[1:2, :]
        l[0:1, at] = l[0:1, at] * shrink + jnp.sum(p, axis=0, keepdims=True)
        h_ref[0:1, :] = shrink
        p_ref[...] = p.astype(BF16)

    def values(i, p_ref, h_ref):
        _, at, chunk = place(i)
        acc[:, at] = acc[:, at] * h_ref[0:1, :] + dot(vt[chunk], p_ref[...])

    scores(0, s_a, w_a)
    scores(1, s_b, w_b)
    probs(0, s_a, w_a, p_a, h_a)

    @pl.loop(1, lax.div(count, 2))
    def _(j):
        i = 2 * j
        values(i - 2, p_a, h_a)
        scores(i, s_a, w_a)
        probs(i - 1, s_b, w_b, p_b, h_b)
        values(i - 1, p_b, h_b)
        scores(i + 1, s_b, w_b)
        probs(i, s_a, w_a, p_a, h_a)

    values(count - 2, p_a, h_a)
    probs(count - 1, s_b, w_b, p_b, h_b)
    values(count - 1, p_b, h_b)


BUFFERS = (
    pltpu.VMEM((ROWS, ROWS), F32),
    pltpu.VMEM((8, ROWS), F32),
    pltpu.VMEM((ROWS, ROWS), BF16),
    pltpu.VMEM((8, ROWS), F32),
) * 2
STATS = (pltpu.VMEM((8, NX * ROWS), F32),) * 2
SPREAD = (pltpu.VMEM((2, ROWS, 256), BF16), pltpu.VMEM((2, 128, ROWS), BF16))


def spread(kv, kk, vt, chunk):
    spread_keys(kv, kk.at[chunk])
    for i in range(4):
        vt[chunk, :, 128 * i : 128 * (i + 1)] = kv[768 + 128 * i : 896 + 128 * i, :]


def own_body(pos, q0, q1, q2, q3, kv, acc, ml, qall, kk, vt, m, l):
    acc[...] = jnp.zeros(acc.shape, F32)
    m[...] = jnp.full(m.shape, FAR_BELOW, F32)
    l[...] = jnp.zeros(l.shape, F32)
    for d, q in enumerate((q0, q1, q2, q3)):
        qall[d, 0:192, :] = q[0:192, :]
        qall[d, 192:256, :] = jnp.zeros((64, ROWS), BF16)
    spread(kv, kk, vt, 0)
    diagonal(qall.at[0], kk.at[0], vt.at[0], acc, m, l)
    x = pos[1]
    for start in (0, 1, 2):

        @pl.when(x == start)
        def _(start=start):
            for d in range(start + 1, NX):
                at = slice(d * ROWS, (d + 1) * ROWS)
                s = dot(kk[0], qall[d]) * FACTOR
                new = jnp.max(s, axis=0, keepdims=True)
                p = jnp.exp2(s - new)
                m[0:1, at] = new
                l[0:1, at] = jnp.sum(p, axis=0, keepdims=True)
                acc[:, at] = dot(vt[0], p.astype(BF16))

    ml[0:1, :] = m[0:1, :]
    ml[1:2, :] = l[0:1, :]
    ml[2:8, :] = jnp.zeros((6, NX * ROWS), F32)


def ring_body(up_step, down_step, final, pos, *refs):
    qall = refs[0]
    n = (up_step > 0) + (down_step > 0)
    chunks = refs[1 : 1 + n]
    acc_in, ml_in = refs[1 + n : 3 + n]
    outs = refs[3 + n :]
    if final:
        packets, acc, (kk, vt, m, l), bufs = outs[:4], outs[4], outs[5:9], outs[9:]
    else:
        (acc, ml), (kk, vt, m, l), bufs = outs[:2], outs[2:6], outs[6:]
    acc[...] = acc_in[...]
    m[0:1, :] = ml_in[0:1, :]
    l[0:1, :] = ml_in[1:2, :]
    z = pos[0]
    count = NX * (z >= up_step).astype(jnp.int32)
    if down_step:
        count = count + NX * (z + down_step >= NZ).astype(jnp.int32)

    @pl.when(z >= up_step)
    def _():
        for chunk, kv in enumerate(chunks):
            spread(kv, kk, vt, chunk)
        attend(count, qall, kk, vt, acc, m, l, (bufs[:4], bufs[4:]))

    if final:
        for d in range(4):
            at = slice(d * ROWS, (d + 1) * ROWS)
            total = jnp.maximum(l[0:1, at], 1e-30)
            packets[d][0:128, :] = (acc[:, at] / total).astype(BF16)
            a, b, e = split3(m[0:1, at] + jnp.log2(total))
            packets[d][128:144, :] = jnp.concatenate([a, b, e, jnp.zeros((13, ROWS), BF16)], axis=0)
    else:
        ml[0:1, :] = m[0:1, :]
        ml[1:2, :] = l[0:1, :]
        ml[2:8, :] = jnp.zeros((6, NX * ROWS), F32)


def out_body(pos, p0, p1, p2, p3, gated, wmem, watt, k0, k1, k2, k3, n0, n1, n2, n3, scr):
    packets = (p0, p1, p2, p3)
    logs = []
    for p in packets:
        s = p[128:144, :].astype(F32)
        logs.append(s[0:1] + s[1:2] + s[2:3])
    top = jnp.maximum(jnp.maximum(logs[0], logs[1]), jnp.maximum(logs[2], logs[3]))
    weights = [jnp.exp2(v - top) for v in logs]
    total = weights[0] + weights[1] + weights[2] + weights[3]
    att = jnp.zeros((128, ROWS), F32)
    for p, w in zip(packets, weights):
        att = att + p[0:128, :].astype(F32) * (w / total)
    att = att.T.astype(BF16)
    scr[...] = (dot(gated[...], wmem[...]) + dot(att, watt[...])).astype(BF16)
    y, c = pos[2], pos[3]
    for d, (keep, send) in enumerate(zip((k0, k1, k2, k3), (n0, n1, n2, n3))):
        yy = lax.rem(y + d, NY)
        keep[...] = scr[pl.ds(pl.multiple_of((2 * yy + c) * 64, 64), 64), :]
        send[...] = scr[pl.ds(pl.multiple_of((2 * yy + 1 - c) * 64, 64), 64), :]


def move(a, axis, pairs):
    return lax.ppermute(a, axis, pairs)


def shift(a, axis, size, by):
    return move(a, axis, [(i, (i + by) % size) for i in range(size)])


def swap(a):
    return shift(a, "c", NC, 1)


def over_tp(piece):
    near = [piece] + [shift(piece, "y", NY, k) for k in (1, 2, 3)]
    pieces = []
    for p in near:
        pieces += [p, swap(p)]
    return pieces


def per_device(
    tokens,
    input_gain,
    weight_query,
    weight_key,
    weight_value,
    weight_outgate,
    weight_ingate,
    weight_forget,
    forget_shift,
    mem_gain,
    query_down_weight,
    latent_down_weight,
    down_rotary,
    query_gain,
    latent_gain,
    query_up_weight,
    key_up_weight,
    value_up_weight,
    out_memory,
    out_attend,
):
    zi, xi = lax.axis_index("z"), lax.axis_index("x")
    yi, ci = lax.axis_index("y"), lax.axis_index("c")
    tp = yi * NC + ci
    pos = jnp.stack([zi, xi, yi, ci]).astype(jnp.int32)

    normed = kernel(norm_body, sds((64, WIDTH), BF16), 2, scalars=False)(
        tokens, input_gain.reshape(1, WIDTH)
    )

    w_gates = jnp.concatenate(
        [
            lax.dynamic_slice_in_dim(weight_ingate, tp, 1, 1).T,
            lax.dynamic_slice_in_dim(weight_forget, tp, 1, 1).T,
            jnp.zeros((14, WIDTH), BF16),
        ],
        axis=0,
    )
    gain_part = lax.dynamic_slice_in_dim(mem_gain, tp * M_V, M_V, 0).astype(F32).reshape(1, M_V)
    shift_row = forget_shift.reshape(1, ROWS)
    qgain, kgain = query_gain.reshape(1, QLAT), latent_gain.reshape(1, KLAT)
    positions = (zi * NX + xi) * ROWS + jnp.arange(ROWS, dtype=jnp.int32)
    inverse = jnp.power(ROTARY_BASE, -jnp.arange(32, dtype=F32) / 32)
    angles = positions.astype(F32)[None, :] * inverse[:, None]
    cos, sin = jnp.cos(angles), jnp.sin(angles)

    pieces = over_tp(normed)
    x_all, rot_raw, latents = kernel(
        latent_body,
        (sds((ROWS, WIDTH), BF16), sds((ROT, ROWS), BF16), sds((160, ROWS), BF16)),
        11,
        far=3,
        scratch=[pltpu.VMEM((224, WIDTH), BF16), pltpu.SemaphoreType.DMA((3,))],
        flops=2 * ROWS * WIDTH * 512,
    )(pos, *pieces, down_rotary.T, query_down_weight.T, latent_down_weight.T)

    lat_pieces = over_tp(latents)

    quarter = sds((72, M_QK), F32)
    q, k, v, og, gates, *states = kernel(
        memory_body,
        (
            sds((ROWS, M_QK), BF16),
            sds((ROWS, M_QK), BF16),
            sds((ROWS, M_V), BF16),
            sds((ROWS, M_V), BF16),
            sds((8, ROWS), F32),
            quarter,
            quarter,
            quarter,
            quarter,
        ),
        7,
        scratch=[pltpu.VMEM((M_V, M_QK), F32)],
        flops=2 * ROWS * WIDTH * 1600,
    )(pos, x_all, weight_query, weight_key, weight_value, weight_outgate, w_gates, shift_row)

    packet = sds((240, ROWS), BF16)
    *qs, kv0 = kernel(
        up_body,
        (packet,) * 4 + (sds((1280, 128), BF16),),
        20,
        scratch=[pltpu.VMEM((QLAT, ROWS), BF16), pltpu.VMEM((KLAT, ROWS), BF16)],
        flops=2 * ROWS * WIDTH * 700,
    )(
        pos,
        *lat_pieces,
        rot_raw,
        query_up_weight.T,
        key_up_weight,
        value_up_weight,
        qgain,
        kgain,
        cos,
        sin,
        *states,
    )

    up, down = [kv0], [kv0]
    for t in range(1, 5):
        up.append(move(up[-1], "z", [(i, i + 1) for i in range(t - 1, NZ - 1)]))
        if t < 4:
            down.append(move(down[-1], "z", [((j + 1) % NZ, j) for j in DOWN[t]]))
    qs = [qs[0]] + [shift(qs[d], "x", NX, d) for d in (1, 2, 3)]

    group, inside = kernel(
        group_body,
        (quarter, sds((NX, 72, M_QK), F32)),
        4,
        scratch=[pltpu.VMEM((NX, 72, M_QK), F32)],
        flops=2 * 10**8,
    )(pos, *qs)

    def from_before(a, by):
        return move(a, "z", [(i, i + by) for i in range(NZ - by)])

    entry = from_before(group, 1)
    window = kernel(scan_one_body, quarter, 2, scalars=False, flops=10**8)(entry, group)
    before = from_before(window, 2)
    window, entry = kernel(
        scan_two_body, (quarter,) * 2, 3, scalars=False, flops=10**8
    )(before, window, entry)
    before = from_before(window, 4)
    carried = kernel(carry_body, (quarter,) * 4, 3, flops=2 * 10**8)(pos, inside, before, entry)
    entered = [carried[0]] + [shift(carried[d], "x", NX, d) for d in (1, 2, 3)]

    state = (sds((128, 4 * ROWS), F32), sds((8, 4 * ROWS), F32))
    tile_flops = 4 * 2 * ROWS * ROWS * 384
    acc, ml, qall = kernel(
        own_body, state + (sds((NX, 256, ROWS), BF16),), 5, flops=tile_flops, scratch=SPREAD + STATS
    )(pos, *qs, kv0)
    share = sds((144, ROWS), BF16)
    for t in range(1, 5):
        last = t == 4
        chunks = [up[t]] + ([] if last else [down[t]])
        n = len(chunks)
        res = kernel(
            functools.partial(ring_body, t, 0 if last else t, last),
            (share,) * 4 if last else state,
            3 + n,
            flops=tile_flops * n,
            scratch=((pltpu.VMEM((128, NX * ROWS), F32),) if last else ()) + SPREAD + STATS + BUFFERS,
            aliases=None if last else {2 + n: 0, 3 + n: 1},
        )(pos, qall, *chunks, acc, ml)
        if last:
            shares = res
        else:
            acc, ml = res

    back = [shares[0]] + [shift(shares[d], "x", NX, -d) for d in (1, 2, 3)]

    cell, ss = kernel(
        cell_body,
        (sds((ROWS, M_V), F32), sds((8, ROWS), F32)),
        8,
        scratch=[pltpu.VMEM((M_V, M_QK), F32)],
        flops=2 * ROWS * WIDTH * 1600,
    )(pos, q, k, v, gates, *entered)
    ss = ss + swap(ss)
    sums = [ss] + [shift(ss, "y", NY, d) for d in (1, 2, 3)]
    gated = kernel(gate_body, sds((ROWS, M_V), BF16), 7, scalars=False, flops=10**9)(
        cell, *sums, gain_part, og
    )

    block = sds((64, WIDTH), BF16)
    res = kernel(
        out_body,
        (block,) * 8,
        7,
        scratch=[pltpu.VMEM((ROWS, WIDTH), BF16)],
        flops=2 * ROWS * WIDTH * 600,
    )(pos, *back, gated, out_memory, out_attend)
    keep, send = res[:4], res[4:]
    got = [swap(s) for s in send]
    pair = [a.astype(F32) + b.astype(F32) for a, b in zip(keep, got)]
    total = pair[0]
    for d in (2, 1, 3):
        total = total + shift(pair[d].astype(BF16), "y", NY, d).astype(F32)
    return total.astype(BF16)


def solution(mesh):
    torus = Mesh(mesh.devices.reshape(NZ, NX, NY, NC), ("z", "x", "y", "c"))
    sp, tp = ("z", "x"), ("y", "c")
    rows = P(("z", "x", "y", "c"), None)
    in_specs = (
        rows,
        P(),
        P(None, tp),
        P(None, tp),
        P(None, tp),
        P(None, tp),
        P(),
        P(),
        P(sp, tp),
        P(),
        P(None, tp),
        P(None, tp),
        P(),
        P(),
        P(),
        P(None, tp),
        P(None, tp),
        P(None, tp),
        P(tp, None),
        P(tp, None),
    )

    return jax.shard_map(per_device, mesh=torus, in_specs=in_specs, out_specs=rows, check_vma=False)
```

```python
import functools

import jax
import jax.numpy as jnp
from jax import lax
from jax.experimental import pallas as pl
from jax.experimental.pallas import tpu as pltpu
from jax.sharding import Mesh
from jax.sharding import PartitionSpec as P

MEMORY_HEADS = 8
M_QK = 128
M_V = 256
NOPE = 128
ROT = 64
QLAT = 768
KLAT = 512
ROWS = 512
WIDTH = 2048
EPS = 1e-06
SOFTCAP = 15.0
ROTARY_BASE = 10000.0
FAR_BELOW = -1e30
LOG2E = 1.4426950408889634
F32 = jnp.float32
BF16 = jnp.bfloat16
NZ, NX, NY, NC = 8, 4, 4, 2


def dot(a, b, dims=((1,), (0,))):
    return lax.dot_general(a, b, (dims, ((), ())), preferred_element_type=F32)


def split2(a):
    hi = a.astype(BF16)
    return hi, (a - hi.astype(F32)).astype(BF16)


def split3(a):
    hi = a.astype(BF16)
    rest = a - hi.astype(F32)
    mid = rest.astype(BF16)
    return hi, mid, (rest - mid.astype(F32)).astype(BF16)


def vmem():
    return pl.BlockSpec(memory_space=pltpu.VMEM)


def smem():
    return pl.BlockSpec(memory_space=pltpu.SMEM)


def kernel(body, outs, n_in, scratch=(), flops=0, scalars=True, aliases=None, far=0):
    specs = ([smem()] if scalars else []) + [vmem()] * (n_in - far)
    specs += [pl.BlockSpec(memory_space=pl.ANY)] * far
    return pl.pallas_call(
        body,
        out_shape=outs,
        in_specs=specs,
        out_specs=jax.tree.map(lambda _: vmem(), outs),
        scratch_shapes=list(scratch),
        input_output_aliases=aliases or {},
        compiler_params=pltpu.CompilerParams(vmem_limit_bytes=14 * 1024 * 1024),
        cost_estimate=pl.CostEstimate(flops=flops, bytes_accessed=0, transcendentals=0),
    )


def sds(shape, dtype):
    return jax.ShapeDtypeStruct(shape, dtype)


def norm_body(tokens, gain, out):
    t = tokens[...].astype(F32)
    scale = lax.rsqrt(jnp.mean(t * t, axis=-1, keepdims=True) + EPS)
    out[...] = (t * scale * gain[...].astype(F32)).astype(BF16)


def prepare_body(pos, w_rot, w_q, w_k, wk, wv, qgain, kgain, cos, sin, wg, mgain, w_out, wkv_out, qcol, kcol):
    w_out[0:64, :] = w_rot[...]
    w_out[64:160, :] = w_q[...]
    w_out[160:224, :] = w_k[...]
    both = jnp.concatenate([wk[...].astype(F32), wv[...].astype(F32)], axis=1)
    wkv_out[...] = both.T.astype(BF16)
    qcol[...] = jnp.broadcast_to(qgain[...], (8, QLAT)).T
    kcol[...] = jnp.broadcast_to(kgain[...], (8, KLAT)).T


def latent_body(pos, *refs):
    pieces, (w, x_out, rot_out, lat_out) = refs[:8], refs[8:]
    y, c = pos[2], pos[3]
    for k in range(NY):
        yy = lax.rem(y + NY - k, NY)
        for side in range(NC):
            cc = c if side == 0 else 1 - c
            at = pl.multiple_of((2 * yy + cc) * 64, 64)
            x_out[pl.ds(at, 64), :] = pieces[2 * k + side][...]
    lat_t = dot(w[...], x_out[...], ((1,), (1,)))
    rot_out[...] = lat_t[0:ROT].astype(BF16)
    lat_out[...] = lat_t[ROT : ROT + 160].astype(BF16)


def memory_body(pos, x_ref, wq, wk, wv, wo, wg, shift, q_out, k_out, v_out, og_out, gates_out, s0, s1, s2, s3, c_scr):
    xx = x_ref[...]
    pre = dot(wg[...], xx, ((1,), (1,)))
    in_gate = SOFTCAP * jnp.tanh(pre[0:1] / SOFTCAP)
    f = SOFTCAP * jnp.tanh((pre[1:2] + shift[...]) / SOFTCAP)
    log_forget = jnp.minimum(f, 0.0) - jnp.log1p(jnp.exp(-jnp.abs(f)))
    row = lax.broadcasted_iota(jnp.int32, (ROWS, ROWS), 0)
    col = lax.broadcasted_iota(jnp.int32, (ROWS, ROWS), 1)
    upper = (row <= col).astype(BF16)
    parts = split3(jnp.broadcast_to(log_forget, (16, ROWS)))
    cum = (dot(parts[0], upper) + dot(parts[1], upper) + dot(parts[2], upper))[0:1]
    pack = jnp.concatenate([cum, in_gate, jnp.zeros((6, ROWS), F32)], axis=0)
    gates_out[...] = pack
    cols = pack.T
    total = cum[:, ROWS - 1 : ROWS]
    weight = jnp.exp(total - cols[:, 0:1] + cols[:, 1:2])
    qk = dot(xx, jnp.concatenate([wq[...], wk[...]], axis=1))
    q_out[...] = qk[:, :M_QK].astype(BF16)
    k = qk[:, M_QK:].astype(BF16)
    k_out[...] = k
    v = dot(xx, wv[...]).astype(BF16)
    v_out[...] = v
    og_out[...] = dot(xx, wo[...]).astype(BF16)
    kw = k.astype(F32) * (M_QK**-0.5) * weight
    a, b, e = split3(kw)
    zero = ((0,), (0,))
    c_scr[...] = dot(v, a, zero) + dot(v, b, zero) + dot(v, e, zero)
    normal = jnp.sum(kw, axis=0, keepdims=True)
    tail = jnp.concatenate(
        [normal, jnp.broadcast_to(total, (1, M_QK)), jnp.zeros((6, M_QK), F32)], axis=0
    )
    for d, ref in enumerate((s0, s1, s2, s3)):
        at = pl.multiple_of(lax.rem(pos[1] + d, NX) * 64, 64)
        ref[0:64, :] = c_scr[pl.ds(at, 64), :]
        ref[64:72, :] = tail


def chain(earlier, later):
    row = lax.broadcasted_iota(jnp.int32, (72, M_QK), 0)
    return jnp.where(row == 65, earlier, jnp.exp(later[65:66]) * earlier) + later


def group_body(pos, r0, r1, r2, r3, group_out, inside_out, scr):
    for d, ref in enumerate((r0, r1, r2, r3)):
        scr[lax.rem(pos[1] + NX - d, NX)] = ref[...]
    run = jnp.zeros((72, M_QK), F32)
    for k in range(NX):
        inside_out[k] = run
        run = chain(run, scr[k])
    group_out[...] = run


def scan_one_body(pos, before, group, window_out, entry_out):
    entry = jnp.where(pos[0] >= 1, before[...], 0.0)
    entry_out[...] = entry
    window_out[...] = chain(entry, group[...])


def scan_two_body(pos, before, window, entry, window_out, entry_out):
    earlier = jnp.where(pos[0] >= 2, before[...], 0.0)
    window_out[...] = chain(earlier, window[...])
    entry_out[...] = chain(earlier, entry[...])


def carry_body(pos, inside, before, entry, o0, o1, o2, o3):
    run = chain(jnp.where(pos[0] >= 4, before[...], 0.0), entry[...])
    for d, ref in enumerate((o0, o1, o2, o3)):
        ref[...] = chain(run, inside[lax.rem(pos[1] + d, NX)])


def cell_body(pos, q_ref, k_ref, v_ref, gates, r0, r1, r2, r3, cell_out, ss_out, c_scr):
    for d, ref in enumerate((r0, r1, r2, r3)):
        at = pl.multiple_of(lax.rem(pos[1] + NX - d, NX) * 64, 64)
        c_scr[pl.ds(at, 64), :] = ref[0:64, :]
    normal = r0[64:65, :]
    state = c_scr[...]
    c3 = split3(state)
    pack = gates[...]
    cum_row = pack[0:1]
    in_row = pack[1:2]
    cols = pack.T
    size = 128
    for t in range(ROWS // size):
        lo, hi = t * size, (t + 1) * size
        qt = q_ref[lo:hi, :]
        cum_col = cols[lo:hi, 0:1]
        scores = dot(qt, k_ref[0:hi, :], ((1,), (1,))) * (M_QK**-0.5)
        logw = cum_col - cum_row[:, 0:hi] + in_row[:, 0:hi]
        row = lax.broadcasted_iota(jnp.int32, (size, hi), 0) + lo
        col = lax.broadcasted_iota(jnp.int32, (size, hi), 1)
        weights = jnp.exp(jnp.where(col <= row, logw, FAR_BELOW))
        aff = scores * weights
        across = jnp.exp(cum_col)
        den = jnp.sum(aff, axis=1, keepdims=True) + across * jnp.sum(
            qt.astype(F32) * normal, axis=1, keepdims=True
        )
        a, b = split2(aff)
        vv = v_ref[0:hi, :]
        num = dot(a, vv) + dot(b, vv)
        nt = ((1,), (1,))
        inter = dot(qt, c3[0], nt) + dot(qt, c3[1], nt) + dot(qt, c3[2], nt)
        cell = (num + across * inter) / jnp.maximum(jnp.abs(den), 1.0)
        cell_out[lo:hi, :] = cell
        ss = jnp.sum(cell * cell, axis=1, keepdims=True)
        ss_out[:, lo:hi] = jnp.broadcast_to(ss, (size, 128)).T[0:8]


def gate_body(cell, t0, t1, t2, t3, gain, og, out):
    total = t0[...] + t1[...] + t2[...] + t3[...]
    scale = lax.rsqrt(total / (MEMORY_HEADS * M_V) + EPS)
    col = scale.T[:, 0:1]
    gated = cell[...] * col * gain[...]
    out[...] = (gated * jax.nn.sigmoid(og[...].astype(F32))).astype(BF16)


def up_body(pos, *refs):
    pieces = refs[:8]
    rot_raw, wq, wkv, qgain, kgain, cos, sin, q_out, kv_out, ql, kl = refs[8:]
    y, c = pos[2], pos[3]
    for k in range(NY):
        yy = lax.rem(y + NY - k, NY)
        for side in range(NC):
            cc = c if side == 0 else 1 - c
            index = 2 * yy + cc
            piece = pieces[2 * k + side]
            ql[pl.ds(pl.multiple_of(index * 96, 32), 96), :] = piece[0:96, :]
            kl[pl.ds(pl.multiple_of(index * 64, 64), 64), :] = piece[96:160, :]

    def turn(u):
        u1, u2 = u[0:32], u[32:64]
        cc, ss = cos[...], sin[...]
        return jnp.concatenate([u1 * cc - u2 * ss, u2 * cc + u1 * ss], axis=0)

    kf = kl[...].astype(F32)
    nk = kf * lax.rsqrt(jnp.mean(kf * kf, axis=0, keepdims=True) + EPS) * kgain[:, 0:1]
    kv = dot(wkv[...], nk.astype(BF16))
    key_rot = turn(rot_raw[...].astype(F32))
    keys = jnp.concatenate([kv[0:NOPE], key_rot, jnp.zeros((64, ROWS), F32)], axis=0).T
    kv_out[0:512, :] = keys[:, 0:NOPE].astype(BF16)
    rot = keys[:, NOPE:]
    kv_out[512:768, :] = (rot[0:256] + pltpu.roll(rot[256:512], 64, 1)).astype(BF16)
    for i in range(4):
        kv_out[768 + 128 * i : 896 + 128 * i, :] = kv[NOPE:, 128 * i : 128 * (i + 1)].astype(BF16)
    qf = ql[...].astype(F32)
    nq = qf * lax.rsqrt(jnp.mean(qf * qf, axis=0, keepdims=True) + EPS) * qgain[:, 0:1]
    qt = dot(wq[...], nq.astype(BF16)).astype(BF16)
    q_out[0:NOPE, :] = qt[0:NOPE]
    q_out[NOPE:, :] = turn(qt[NOPE:].astype(F32)).astype(BF16)


FACTOR = (NOPE + ROT) ** -0.5 * LOG2E


def spread_keys(kv, kk):
    kk[:, 0:NOPE] = kv[0:512, :]
    rot = kv[512:768, :].astype(F32)
    lane = lax.broadcasted_iota(jnp.int32, (256, 128), 1)
    kk[0:256, NOPE:] = jnp.where(lane < ROT, rot, 0.0).astype(BF16)
    kk[256:512, NOPE:] = jnp.where(lane < ROT, pltpu.roll(rot, 64, 1), 0.0).astype(BF16)


def diagonal(q, kk, vt, acc, m, l):
    for h in range(2):
        lo, hi = h * 256, (h + 1) * 256
        s = dot(kk[0:hi, :], q[:, lo:hi]) * FACTOR
        key = lax.broadcasted_iota(jnp.int32, (hi, 256), 0)
        qry = lax.broadcasted_iota(jnp.int32, (hi, 256), 1) + lo
        s = jnp.where(key <= qry, s, FAR_BELOW)
        new = jnp.max(s, axis=0, keepdims=True)
        p = jnp.exp2(s - new)
        m[0:1, lo:hi] = new
        l[0:1, lo:hi] = jnp.sum(p, axis=0, keepdims=True)
        acc[:, lo:hi] = dot(vt[:, 0:hi], p.astype(BF16))


def attend(count, qall, kk, vt, acc, m, l, bufs):
    (s_a, w_a, p_a, h_a), (s_b, w_b, p_b, h_b) = bufs

    def place(i):
        d = lax.rem(i, NX)
        return d, pl.ds(pl.multiple_of(d * ROWS, ROWS), ROWS), lax.div(i, NX)

    def scores(i, s_ref, w_ref):
        d, at, chunk = place(i)
        s = dot(kk[chunk], qall[d]) * FACTOR
        old = m[0:1, at]
        new = jnp.maximum(old, jnp.max(s, axis=0, keepdims=True))
        s_ref[...] = s
        w_ref[0:1, :] = new
        w_ref[1:2, :] = jnp.exp2(old - new)
        m[0:1, at] = new

    def probs(i, s_ref, w_ref, p_ref, h_ref):
        _, at, _ = place(i)
        p = jnp.exp2(s_ref[...] - w_ref[0:1, :])
        shrink = w_ref[1:2, :]
        l[0:1, at] = l[0:1, at] * shrink + jnp.sum(p, axis=0, keepdims=True)
        h_ref[0:1, :] = shrink
        p_ref[...] = p.astype(BF16)

    def values(i, p_ref, h_ref):
        _, at, chunk = place(i)
        acc[:, at] = acc[:, at] * h_ref[0:1, :] + dot(vt[chunk], p_ref[...])

    scores(0, s_a, w_a)
    scores(1, s_b, w_b)
    probs(0, s_a, w_a, p_a, h_a)

    @pl.loop(1, lax.div(count, 2))
    def _(j):
        i = 2 * j
        values(i - 2, p_a, h_a)
        scores(i, s_a, w_a)
        probs(i - 1, s_b, w_b, p_b, h_b)
        values(i - 1, p_b, h_b)
        scores(i + 1, s_b, w_b)
        probs(i, s_a, w_a, p_a, h_a)

    values(count - 2, p_a, h_a)
    probs(count - 1, s_b, w_b, p_b, h_b)
    values(count - 1, p_b, h_b)


BUFFERS = (
    pltpu.VMEM((ROWS, ROWS), F32),
    pltpu.VMEM((8, ROWS), F32),
    pltpu.VMEM((ROWS, ROWS), BF16),
    pltpu.VMEM((8, ROWS), F32),
) * 2
STATS = (pltpu.VMEM((8, NX * ROWS), F32),) * 2
SPREAD = (pltpu.VMEM((2, ROWS, 256), BF16), pltpu.VMEM((2, 128, ROWS), BF16))


def spread(kv, kk, vt, chunk):
    spread_keys(kv, kk.at[chunk])
    for i in range(4):
        vt[chunk, :, 128 * i : 128 * (i + 1)] = kv[768 + 128 * i : 896 + 128 * i, :]


def own_body(pos, q0, q1, q2, q3, kv, acc, ml, qall, kk, vt, m, l):
    acc[...] = jnp.zeros(acc.shape, F32)
    m[...] = jnp.full(m.shape, FAR_BELOW, F32)
    l[...] = jnp.zeros(l.shape, F32)
    for d, q in enumerate((q0, q1, q2, q3)):
        qall[d, 0:192, :] = q[0:192, :]
        qall[d, 192:256, :] = jnp.zeros((64, ROWS), BF16)
    spread(kv, kk, vt, 0)
    diagonal(qall.at[0], kk.at[0], vt.at[0], acc, m, l)

    @pl.loop(pos[1] + 1, NX)
    def _(d):
        at = pl.ds(pl.multiple_of(d * ROWS, ROWS), ROWS)
        s = dot(kk[0], qall[d]) * FACTOR
        new = jnp.max(s, axis=0, keepdims=True)
        p = jnp.exp2(s - new)
        m[0:1, at] = new
        l[0:1, at] = jnp.sum(p, axis=0, keepdims=True)
        acc[:, at] = dot(vt[0], p.astype(BF16))

    ml[0:1, :] = m[0:1, :]
    ml[1:2, :] = l[0:1, :]
    ml[2:8, :] = jnp.zeros((6, NX * ROWS), F32)


def ring_body(up_step, down_step, final, pos, *refs):
    qall = refs[0]
    n = (up_step > 0) + (down_step > 0)
    chunks = refs[1 : 1 + n]
    acc_in, ml_in = refs[1 + n : 3 + n]
    outs = refs[3 + n :]
    if final:
        packets, acc, (kk, vt, m, l), bufs = outs[:4], outs[4], outs[5:9], outs[9:]
    else:
        (acc, ml), (kk, vt, m, l), bufs = outs[:2], outs[2:6], outs[6:]
    acc[...] = acc_in[...]
    m[0:1, :] = ml_in[0:1, :]
    l[0:1, :] = ml_in[1:2, :]
    z = pos[0]
    count = NX * (z >= up_step).astype(jnp.int32)
    if down_step:
        count = count + NX * (z + down_step >= NZ).astype(jnp.int32)

    @pl.when(z >= up_step)
    def _():
        for chunk, kv in enumerate(chunks):
            spread(kv, kk, vt, chunk)
        attend(count, qall, kk, vt, acc, m, l, (bufs[:4], bufs[4:]))

    if final:
        for d in range(4):
            at = slice(d * ROWS, (d + 1) * ROWS)
            total = jnp.maximum(l[0:1, at], 1e-30)
            packets[d][0:128, :] = (acc[:, at] / total).astype(BF16)
            a, b, e = split3(m[0:1, at] + jnp.log2(total))
            packets[d][128:144, :] = jnp.concatenate([a, b, e, jnp.zeros((13, ROWS), BF16)], axis=0)
    else:
        ml[0:1, :] = m[0:1, :]
        ml[1:2, :] = l[0:1, :]
        ml[2:8, :] = jnp.zeros((6, NX * ROWS), F32)


def project_blocks(y, c, gated, att, wmem, watt, outs):
    spots = [pl.multiple_of((2 * lax.rem(y + d, NY) + c) * 64, 64) for d in range(NY)]
    g = jnp.concatenate([gated[pl.ds(at, 64), :] for at in spots], axis=0)
    a = jnp.concatenate([att[pl.ds(at, 64), :] for at in spots], axis=0)
    partial = (dot(g, wmem[...]) + dot(a, watt[...])).astype(BF16)
    for d, out in enumerate(outs):
        out[...] = partial[64 * d : 64 * (d + 1), :]


def send_body(pos, p0, p1, p2, p3, gated, wmem, watt, att_out, n0, n1, n2, n3):
    packets = (p0, p1, p2, p3)
    logs = []
    for p in packets:
        s = p[128:144, :].astype(F32)
        logs.append(s[0:1] + s[1:2] + s[2:3])
    top = jnp.maximum(jnp.maximum(logs[0], logs[1]), jnp.maximum(logs[2], logs[3]))
    weights = [jnp.exp2(v - top) for v in logs]
    total = weights[0] + weights[1] + weights[2] + weights[3]
    att = jnp.zeros((128, ROWS), F32)
    for p, w in zip(packets, weights):
        att = att + p[0:128, :].astype(F32) * (w / total)
    att_out[...] = att.T.astype(BF16)
    project_blocks(pos[2], 1 - pos[3], gated, att_out, wmem, watt, (n0, n1, n2, n3))


def keep_body(pos, att, gated, wmem, watt, k0, k1, k2, k3):
    project_blocks(pos[2], pos[3], gated, att, wmem, watt, (k0, k1, k2, k3))


def shift(a, axis, size, by):
    return lax.ppermute(a, axis, [(i, (i + by) % size) for i in range(size)])


def swap(a):
    return shift(a, "c", NC, 1)


def over_tp(piece):
    near = [piece] + [shift(piece, "y", NY, k) for k in (1, 2, 3)]
    pieces = []
    for p in near:
        pieces += [p, swap(p)]
    return pieces


def per_device(
    tokens,
    input_gain,
    weight_query,
    weight_key,
    weight_value,
    weight_outgate,
    weight_ingate,
    weight_forget,
    forget_shift,
    mem_gain,
    query_down_weight,
    latent_down_weight,
    down_rotary,
    query_gain,
    latent_gain,
    query_up_weight,
    key_up_weight,
    value_up_weight,
    out_memory,
    out_attend,
):
    zi, xi = lax.axis_index("z"), lax.axis_index("x")
    yi, ci = lax.axis_index("y"), lax.axis_index("c")
    tp = yi * NC + ci
    pos = jnp.stack([zi, xi, yi, ci]).astype(jnp.int32)

    normed = kernel(norm_body, sds((64, WIDTH), BF16), 2, scalars=False)(
        tokens, input_gain.reshape(1, WIDTH)
    )

    w_gates = jnp.concatenate(
        [
            lax.dynamic_slice_in_dim(weight_ingate, tp, 1, 1).T,
            lax.dynamic_slice_in_dim(weight_forget, tp, 1, 1).T,
            jnp.zeros((14, WIDTH), BF16),
        ],
        axis=0,
    )
    gain_part = lax.dynamic_slice_in_dim(mem_gain, tp * M_V, M_V, 0).astype(F32).reshape(1, M_V)
    shift_row = forget_shift.reshape(1, ROWS)
    qgain, kgain = query_gain.reshape(1, QLAT), latent_gain.reshape(1, KLAT)
    positions = (zi * NX + xi) * ROWS + jnp.arange(ROWS, dtype=jnp.int32)
    inverse = jnp.power(ROTARY_BASE, -jnp.arange(32, dtype=F32) / 32)
    angles = positions.astype(F32)[None, :] * inverse[:, None]
    cos, sin = jnp.cos(angles), jnp.sin(angles)

    w_lat, w_kv, qcol, kcol = kernel(
        prepare_body,
        (sds((224, WIDTH), BF16), sds((256, KLAT), BF16), sds((QLAT, 8), F32), sds((KLAT, 8), F32)),
        11,
        far=4,
    )(
        pos,
        down_rotary.T,
        query_down_weight.T,
        latent_down_weight.T,
        key_up_weight,
        value_up_weight,
        qgain,
        kgain,
        cos,
        sin,
        w_gates,
        gain_part,
    )

    pieces = over_tp(normed)
    x_all, rot_raw, latents = kernel(
        latent_body,
        (sds((ROWS, WIDTH), BF16), sds((ROT, ROWS), BF16), sds((160, ROWS), BF16)),
        9,
        flops=2 * ROWS * WIDTH * 512,
    )(pos, *pieces, w_lat)

    lat_pieces = over_tp(latents)

    quarter = sds((72, M_QK), F32)
    q, k, v, og, gates, *states = kernel(
        memory_body,
        (
            sds((ROWS, M_QK), BF16),
            sds((ROWS, M_QK), BF16),
            sds((ROWS, M_V), BF16),
            sds((ROWS, M_V), BF16),
            sds((8, ROWS), F32),
            quarter,
            quarter,
            quarter,
            quarter,
        ),
        7,
        scratch=[pltpu.VMEM((M_V, M_QK), F32)],
        flops=2 * ROWS * WIDTH * 1600,
    )(pos, x_all, weight_query, weight_key, weight_value, weight_outgate, w_gates, shift_row)

    q_t, kv0 = kernel(
        up_body,
        (sds((192, ROWS), BF16), sds((1280, 128), BF16)),
        15,
        scratch=[pltpu.VMEM((QLAT, ROWS), BF16), pltpu.VMEM((KLAT, ROWS), BF16)],
        flops=2 * ROWS * WIDTH * 700,
    )(pos, *lat_pieces, rot_raw, query_up_weight.T, w_kv, qcol, kcol, cos, sin)

    up, down = [kv0], [kv0]
    for t in range(1, 5):
        up.append(shift(up[-1], "z", NZ, 1))
        if t < 4:
            down.append(shift(down[-1], "z", NZ, -1))
    arrived = [states[0]] + [shift(states[d], "x", NX, d) for d in (1, 2, 3)]
    qs = [q_t] + [shift(q_t, "x", NX, d) for d in (1, 2, 3)]

    group, inside = kernel(
        group_body,
        (quarter, sds((NX, 72, M_QK), F32)),
        4,
        scratch=[pltpu.VMEM((NX, 72, M_QK), F32)],
        flops=2 * 10**8,
    )(pos, *arrived)

    def from_before(a, by):
        return shift(a, "z", NZ, by)

    window, entry = kernel(scan_one_body, (quarter,) * 2, 2, flops=10**8)(
        pos, from_before(group, 1), group
    )
    before = from_before(window, 2)
    window, entry = kernel(scan_two_body, (quarter,) * 2, 3, flops=10**8)(
        pos, before, window, entry
    )
    before = from_before(window, 4)
    carried = kernel(carry_body, (quarter,) * 4, 3, flops=2 * 10**8)(
        pos, inside, before, entry
    )
    entered = [carried[0]] + [shift(carried[d], "x", NX, d) for d in (1, 2, 3)]

    state = (sds((128, 4 * ROWS), F32), sds((8, 4 * ROWS), F32))
    tile_flops = 4 * 2 * ROWS * ROWS * 384
    acc, ml, qall = kernel(
        own_body,
        state + (sds((NX, 256, ROWS), BF16),),
        5,
        flops=tile_flops,
        scratch=SPREAD + STATS,
    )(pos, *qs, kv0)
    share = sds((144, ROWS), BF16)
    for t in range(1, 5):
        last = t == 4
        chunks = [up[t]] + ([] if last else [down[t]])
        n = len(chunks)
        res = kernel(
            functools.partial(ring_body, t, 0 if last else t, last),
            (share,) * 4 if last else state,
            3 + n,
            flops=tile_flops * n,
            scratch=((pltpu.VMEM((128, NX * ROWS), F32),) if last else ()) + SPREAD + STATS + BUFFERS,
            aliases=None if last else {2 + n: 0, 3 + n: 1},
        )(pos, qall, *chunks, acc, ml)
        if last:
            shares = res
        else:
            acc, ml = res

    back = [shares[0]] + [shift(shares[d], "x", NX, -d) for d in (1, 2, 3)]

    cell, ss = kernel(
        cell_body,
        (sds((ROWS, M_V), F32), sds((8, ROWS), F32)),
        8,
        scratch=[pltpu.VMEM((M_V, M_QK), F32)],
        flops=2 * ROWS * WIDTH * 1600,
    )(pos, q, k, v, gates, *entered)
    ss = ss + swap(ss)
    sums = [ss] + [shift(ss, "y", NY, d) for d in (1, 2, 3)]
    gated = kernel(gate_body, sds((ROWS, M_V), BF16), 7, scalars=False, flops=10**9)(
        cell, *sums, gain_part, og
    )

    block = sds((64, WIDTH), BF16)
    att, *send = kernel(
        send_body, (sds((ROWS, 128), BF16),) + (block,) * 4, 7, flops=ROWS * WIDTH * 600
    )(pos, *back, gated, out_memory, out_attend)
    keep = kernel(keep_body, (block,) * 4, 4, flops=ROWS * WIDTH * 600)(
        pos, att, gated, out_memory, out_attend
    )
    got = [swap(s) for s in send]
    pair = [a.astype(F32) + b.astype(F32) for a, b in zip(keep, got)]
    total = pair[0]
    for d in (2, 1, 3):
        total = total + shift(pair[d].astype(BF16), "y", NY, d).astype(F32)
    return total.astype(BF16)


def solution(mesh):
    torus = Mesh(mesh.devices.reshape(NZ, NX, NY, NC), ("z", "x", "y", "c"))
    sp, tp = ("z", "x"), ("y", "c")
    rows = P(("z", "x", "y", "c"), None)
    in_specs = (
        rows,
        P(),
        P(None, tp),
        P(None, tp),
        P(None, tp),
        P(None, tp),
        P(),
        P(),
        P(sp, tp),
        P(),
        P(None, tp),
        P(None, tp),
        P(),
        P(),
        P(),
        P(None, tp),
        P(None, tp),
        P(None, tp),
        P(tp, None),
        P(tp, None),
    )

    return jax.shard_map(
        per_device, mesh=torus, in_specs=in_specs, out_specs=rows, check_vma=False
    )
```
